128 devices in a mesh: rep: 2 (over z_hi), fs: 32 (over z_lo, y, x), tp: 2 (over core).
Axes of the slice: x: 4, y: 4, z: 4 (z_hi: 2, z_lo: 2; z = z_hi * 2 + z_lo), core: 2. Of those that a mesh axis runs over, the one named last changes fastest.
Arguments:
- tokens: bfloat16 [49152, 2048], P(('rep', 'fs'), 'tp'), may hold values from -6 to 6
- first_norm_gain: bfloat16 [2048], replicated, may hold values from 0.099609375 to 1.8984375
- query_projection_weight: bfloat16 [2048, 512], P('fs', 'tp'), may hold values from -0.125 to 0.125
- key_projection_weight: bfloat16 [2048, 512], P('fs', 'tp'), may hold values from -0.125 to 0.125
- value_projection_weight: bfloat16 [2048, 1024], P('fs', 'tp'), may hold values from -0.125 to 0.125
- output_gate_weight: bfloat16 [2048, 1024], P('fs', 'tp'), may hold values from -0.125 to 0.125
- decay_projection_weight: bfloat16 [2048, 512], P('fs', 'tp'), may hold values from -0.375 to 0.375
- fading_shift_vector: float32 [512], P('tp'), may hold values from -1 to 4
- added_fading_exponent: float32 [49152, 512], P(('rep', 'fs'), 'tp'), may hold values from -0.7 to 0
- per_head_gain: bfloat16 [128], replicated, may hold values from 0.099609375 to 1.8984375
- mixer_result_matrix: bfloat16 [1024, 2048], P('tp', 'fs'), may hold values from -0.1875 to 0.1875
- second_norm_gain: bfloat16 [2048], replicated, may hold values from 0.099609375 to 1.8984375
- up_linear_weight: bfloat16 [2048, 3072], P('fs', 'tp'), may hold values from -0.125 to 0.125
- up_gating_weight: bfloat16 [2048, 3072], P('fs', 'tp'), may hold values from -0.125 to 0.125
- depthwise_taps: bfloat16 [2, 3, 3072], P(None, None, 'tp'), may hold values from -3.5 to 3.5
- depthwise_bias: bfloat16 [2, 3072], P(None, 'tp'), may hold values from -3 to 3
- down_projection_weight: bfloat16 [3072, 2048], P('tp', 'fs'), may hold values from -0.109375 to 0.109375
Outputs:
- mixed: bfloat16 [49152, 2048], P(('rep', 'fs'), 'tp')
The draws below stay inside these ranges and needn't reach their ends.
All inputs are finite; a program needn't handle non-finite values.
Results may differ from the reference program's by a relative error of at most 0.018.
Values may be sent and summed in bfloat16 or wider, within the bound.
A program may use at most 128 MiB of HBM per device.

```python
import math
import jax
import jax.numpy as jnp
from jax import lax

D = 2048
HEADS = 8
KEY_DIM = 64
VALUE_DIM = 128
FF = 3072
KERNEL = 3
BLOCK = 64
SEQ_LEN = 256
TOKENS = 49152
N_TP = 2


def draw_added_fading_exponent(key, part):
    place_key, level_key = jax.random.split(jax.random.fold_in(key, 7))
    struck = jax.random.randint(place_key, (TOKENS, 1), 0, 64) == 0
    strength = jax.random.uniform(level_key, (TOKENS, HEADS * KEY_DIM), jnp.float32, math.log(0.5), math.log(0.8))
    return jnp.where(struck, strength, 0.0).astype(jnp.float32)


def levels(own_key, extent, pieces, smallest, largest):
    def one(dim, blocks):
        steps = jax.random.uniform(jax.random.fold_in(jax.random.fold_in(own_key, 6), dim), (blocks,), jnp.float32, smallest / len(pieces), largest / len(pieces))
        return jnp.repeat(jnp.exp(steps), extent[dim] // blocks).reshape((-1,) + (1,) * (len(extent) - dim - 1))

    level = one(*pieces[0])
    for cut in pieces[1:]:
        level = level * one(*cut)
    return level


def noise(stream_key, extent, deviation, most, cuts=(), kind=jnp.bfloat16):
    factor_of = levels(stream_key, extent, cuts, -0.22, 0.18) if cuts else 1.0
    drawn = jax.random.normal(stream_key, extent, jnp.float32) * deviation * factor_of
    return jnp.minimum(jnp.maximum(drawn, -most), most).astype(kind)


def setup_inputs(seed: int = 0) -> dict:
    key_list = jax.random.split(jax.random.key(seed), 18)
    tokens = noise(key_list[0], (TOKENS, D), 1.0, 6.0, ((0, 64), (1, 2)))
    first_norm_gain = jnp.clip(1.0 + 0.18 * jax.random.normal(key_list[1], (D,), jnp.float32), 0.099609375, 1.8984375).astype(jnp.bfloat16)
    query_projection_weight = noise(key_list[2], (D, HEADS * KEY_DIM), D ** -0.5, 0.125, ((0, 32), (1, 2)))
    key_projection_weight = noise(key_list[3], (D, HEADS * KEY_DIM), D ** -0.5, 0.125, ((0, 32), (1, 2)))
    value_projection_weight = noise(key_list[4], (D, HEADS * VALUE_DIM), D ** -0.5, 0.125, ((0, 32), (1, 2)))
    output_gate_weight = noise(key_list[5], (D, HEADS * VALUE_DIM), D ** -0.5, 0.125, ((0, 32), (1, 2)))
    decay_projection_weight = noise(key_list[6], (D, HEADS * KEY_DIM), (D // 9) ** -0.5, 0.375, ((0, 32), (1, 2)))
    fading_shift_vector = jnp.clip(-1.0 + 5.0 * jax.random.uniform(key_list[7], (HEADS * KEY_DIM,), jnp.float32) ** levels(key_list[7], (HEADS * KEY_DIM,), ((0, 2),), -0.2, 0.2), -1.0, 4.0)
    added_fading_exponent = draw_added_fading_exponent(jax.random.fold_in(key_list[17], 71), 0)
    per_head_gain = jnp.clip(1.0 + 0.18 * jax.random.normal(key_list[9], (VALUE_DIM,), jnp.float32), 0.099609375, 1.8984375).astype(jnp.bfloat16)
    mixer_result_matrix = noise(key_list[10], (HEADS * VALUE_DIM, D), (HEADS * VALUE_DIM) ** -0.5, 0.1875, ((0, 2), (1, 32)))
    second_norm_gain = jnp.clip(1.0 + 0.18 * jax.random.normal(key_list[11], (D,), jnp.float32), 0.099609375, 1.8984375).astype(jnp.bfloat16)
    up_linear_weight = noise(key_list[12], (D, FF), D ** -0.5, 0.125, ((0, 32), (1, 2)))
    up_gating_weight = noise(key_list[13], (D, FF), D ** -0.5, 0.125, ((0, 32), (1, 2)))
    depthwise_taps = noise(key_list[14], (2, KERNEL, FF), KERNEL ** -0.5, 3.5, ((2, 2),))
    depthwise_bias = noise(key_list[15], (2, FF), 0.5, 3.0, ((1, 2),))
    down_projection_weight = noise(key_list[16], (FF, D), FF ** -0.5, 0.109375, ((0, 2), (1, 32)))
    return dict(tokens=tokens, first_norm_gain=first_norm_gain, query_projection_weight=query_projection_weight, key_projection_weight=key_projection_weight, value_projection_weight=value_projection_weight, output_gate_weight=output_gate_weight, decay_projection_weight=decay_projection_weight, fading_shift_vector=fading_shift_vector, added_fading_exponent=added_fading_exponent, per_head_gain=per_head_gain, mixer_result_matrix=mixer_result_matrix, second_norm_gain=second_norm_gain, up_linear_weight=up_linear_weight, up_gating_weight=up_gating_weight, depthwise_taps=depthwise_taps, depthwise_bias=depthwise_bias, down_projection_weight=down_projection_weight)


norm_eps = 1e-06
fading_sharpness = 16.0

def normalize(source, gain):
    widened = source.astype(jnp.float32)
    scaled = widened * lax.rsqrt(lax.optimization_barrier(jnp.mean(widened * widened, axis=-1, keepdims=True)) + norm_eps)
    return (scaled * gain.astype(jnp.float32)).astype(jnp.bfloat16)

def direction(queries, key_heads, value_heads, fading_exponent):
    sequences, length, head_count, key_depth = queries.shape
    value_depth = value_heads.shape[-1]
    block_count = length // BLOCK
    query_blocks = queries.reshape(sequences, block_count, BLOCK, head_count, key_depth)
    key_blocks = key_heads.reshape(sequences, block_count, BLOCK, head_count, key_depth)
    value_blocks = value_heads.reshape(sequences, block_count, BLOCK, head_count, value_depth)
    cumulative = jnp.cumsum(fading_exponent.reshape(sequences, block_count, BLOCK, head_count, key_depth), axis=2)
    block_total = cumulative[:, :, -1:]
    query_decayed = query_blocks * jnp.exp(cumulative)
    key_inverse = key_blocks * jnp.exp(-cumulative)
    key_carried = key_blocks * jnp.exp(block_total - cumulative)
    lower_mask = jnp.tril(jnp.ones((BLOCK, BLOCK), dtype=bool))
    scores = jnp.einsum('snihd,snjhd->snhij', query_decayed, key_inverse, precision=lax.Precision.HIGHEST)
    scores = jnp.where(lower_mask, scores, 0.0)
    within_block = jnp.einsum('snhij,snjhv->snihv', scores, value_blocks, precision=lax.Precision.HIGHEST)
    increments = jnp.einsum('snchd,snchv->nshdv', key_carried, value_blocks, precision=lax.Precision.HIGHEST)
    carry_decay = jnp.moveaxis(jnp.exp(block_total[:, :, 0]), 1, 0)

    def advance(running, inputs):
        factor, update = inputs
        return (factor[..., None] * running + update, running)
    initial = jnp.zeros((sequences, head_count, key_depth, value_depth), jnp.float32)
    unused, previous = lax.scan(advance, initial, (carry_decay, increments))
    across_blocks = jnp.einsum('snchd,nshdv->snchv', query_decayed, previous, precision=lax.Precision.HIGHEST)
    return (within_block + across_blocks).reshape(sequences, length, head_count, value_depth)

def mixer_heads(queries_raw, keys_raw, values_raw, gates_raw, fading_exponent, per_head_gain):
    row_count = queries_raw.shape[0]
    head_count = values_raw.shape[1] // VALUE_DIM
    key_shape = (row_count // SEQ_LEN, SEQ_LEN, head_count, KEY_DIM)
    value_shape = (row_count // SEQ_LEN, SEQ_LEN, head_count, VALUE_DIM)
    queries = queries_raw.astype(jnp.float32).reshape(key_shape) * KEY_DIM ** (-0.5)
    key_heads = keys_raw.astype(jnp.float32).reshape(key_shape)
    value_heads = values_raw.astype(jnp.float32).reshape(value_shape)
    decay_heads = fading_exponent.reshape(key_shape)
    forward = direction(queries, key_heads, value_heads, decay_heads)
    backward = direction(jnp.flip(queries, 1), jnp.flip(key_heads, 1), jnp.flip(value_heads, 1), jnp.flip(decay_heads, 1))
    attention = forward + jnp.flip(backward, 1)
    scaled = attention * lax.rsqrt(lax.optimization_barrier(jnp.mean(attention * attention, axis=-1, keepdims=True)) + norm_eps)
    scaled = scaled * per_head_gain.astype(jnp.float32)
    merged = scaled.reshape(row_count, head_count * VALUE_DIM)
    return (merged * jax.nn.silu(gates_raw.astype(jnp.float32))).astype(jnp.bfloat16)

def depthwise(linear_out, gated_out, depthwise_taps, depthwise_bias):
    row_count, channels = linear_out.shape

    def smooth(source, taps, offset_bias):
        framed = source.astype(jnp.float32).reshape(row_count // SEQ_LEN, SEQ_LEN, channels)
        tap_count = taps.shape[0]
        leading_zero_fill = tap_count // 2
        padded = jnp.pad(framed, ((0, 0), (leading_zero_fill, tap_count - 1 - leading_zero_fill), (0, 0)))
        result = offset_bias.astype(jnp.float32)
        for shift_index in range(tap_count):
            result = result + padded[:, shift_index:shift_index + SEQ_LEN] * taps[shift_index].astype(jnp.float32)
        return result
    linear_conv = smooth(linear_out, depthwise_taps[0], depthwise_bias[0])
    gate_conv = smooth(gated_out, depthwise_taps[1], depthwise_bias[1])
    return (linear_conv * jax.nn.silu(gate_conv)).astype(jnp.bfloat16).reshape(row_count, channels)

def group_sum(left_side, right_side):
    group_rows = left_side.shape[1] // N_TP
    summed = jnp.zeros((left_side.shape[0], right_side.shape[1]), jnp.float32)
    for member in range(N_TP):
        partial_prod = jnp.dot(left_side[:, member * group_rows:(member + 1) * group_rows], right_side[member * group_rows:(member + 1) * group_rows], preferred_element_type=jnp.float32)
        summed = summed + lax.optimization_barrier(partial_prod.astype(jnp.bfloat16)).astype(jnp.float32)
    return summed

def reference(tokens, first_norm_gain, query_projection_weight, key_projection_weight, value_projection_weight, output_gate_weight, decay_projection_weight, fading_shift_vector, added_fading_exponent, per_head_gain, mixer_result_matrix, second_norm_gain, up_linear_weight, up_gating_weight, depthwise_taps, depthwise_bias, down_projection_weight):
    normed = normalize(tokens, first_norm_gain)
    queries_raw = jnp.dot(normed, query_projection_weight, preferred_element_type=jnp.float32).astype(jnp.bfloat16)
    keys_raw = jnp.dot(normed, key_projection_weight, preferred_element_type=jnp.float32).astype(jnp.bfloat16)
    values_raw = jnp.dot(normed, value_projection_weight, preferred_element_type=jnp.float32).astype(jnp.bfloat16)
    gates_raw = jnp.dot(normed, output_gate_weight, preferred_element_type=jnp.float32).astype(jnp.bfloat16)
    fading_scores_raw = jnp.dot(normed, decay_projection_weight, preferred_element_type=jnp.float32)
    fading_exponent = jax.nn.log_sigmoid(fading_scores_raw + fading_shift_vector) / fading_sharpness + added_fading_exponent
    mixed_heads = mixer_heads(queries_raw, keys_raw, values_raw, gates_raw, fading_exponent, per_head_gain)
    mixer_out = group_sum(mixed_heads, mixer_result_matrix)
    after_mixer = (tokens.astype(jnp.float32) + mixer_out).astype(jnp.bfloat16)
    normed_two = normalize(after_mixer, second_norm_gain)
    linear_out = jnp.dot(normed_two, up_linear_weight, preferred_element_type=jnp.float32).astype(jnp.bfloat16)
    gated_out = jnp.dot(normed_two, up_gating_weight, preferred_element_type=jnp.float32).astype(jnp.bfloat16)
    hidden = depthwise(linear_out, gated_out, depthwise_taps, depthwise_bias)
    channel_out = group_sum(hidden, down_projection_weight)
    return (after_mixer.astype(jnp.float32) + channel_out).astype(jnp.bfloat16)
```

```python
import jax
import jax.numpy as jnp
from jax import lax
from jax.experimental import pallas as pl
from jax.experimental.pallas import tpu as pltpu
from jax.sharding import PartitionSpec as P


LANE = 128
MESH = pl.DeviceIdType.MESH
GROUPS = ((0, (6, 5, 3, 4)), (18, (7, 8, 5, 4)), (42, (4, 4, 2, 2)))
COLS = 54 * LANE
CLASSES = (("x", 1, True), ("y", -1, True), ("x", 1, False), ("y", -1, False))
NSEM = 144


class Gather:
    def __init__(self, full, send_sem, recv_sem):
        self.full, self.send_sem, self.recv_sem = full, send_sem, recv_sem
        rep, fs, self.tp = (lax.axis_index(a) for a in ("rep", "fs", "tp"))
        self.x, self.y, self.l = lax.rem(fs, 4), lax.rem(fs // 4, 4), fs // 16
        self.z = rep * 2 + self.l
        self.ids, self.copies = {}, {}

    def device(self, dim, step):
        x, y, z = self.x, self.y, self.z
        if dim == "x":
            x = lax.rem(x + step + 4, 4)
        elif dim == "y":
            y = lax.rem(y + step + 4, 4)
        else:
            z = lax.rem(z + step + 4, 4)
        return (z // 2, lax.rem(z, 2) * 16 + y * 4 + x, self.tp)

    def neighbours(self):
        return [self.device(d, s) for d in "xyz" for s in (1, -1)] + [
            (self.z // 2, self.l * 16 + self.y * 4 + self.x, 1 - self.tp)
        ]

    def cols(self, g, c):
        at, widths = GROUPS[g]
        return pl.ds((at + sum(widths[:c])) * LANE, widths[c] * LANE)

    def piece(self, g, c, stage, off, half=None, z=None):
        first, _, last = CLASSES[c]
        if z is None:
            zs = pl.ds(self.l, 1) if last else pl.ds(0, 2)
        else:
            zs = pl.ds(z, 1)
        rows = pl.ds(0, 64) if half is None else pl.ds(32 * half, 32)
        dim = first if stage == 1 else ("y" if first == "x" else "x")
        mine = self.x if dim == "x" else self.y
        at = pl.ds(lax.rem(mine + off + 4, 4), 1)
        if stage == 1:
            other = pl.ds(self.y if dim == "x" else self.x, 1)
        else:
            other = pl.ds(0, 4)
        yx = (other, at) if dim == "x" else (at, other)
        return self.full.at[zs, yx[0], yx[1], rows, self.cols(g, c)]

    def copy(self, key, ref, dim, step):
        i = self.ids.setdefault(key, len(self.ids))
        return pltpu.make_async_remote_copy(
            src_ref=ref,
            dst_ref=ref,
            send_sem=self.send_sem.at[i],
            recv_sem=self.recv_sem.at[i],
            device_id=self.device(dim, step),
            device_id_type=MESH,
        )

    def send(self, key, ref, dim, step):
        copy = self.copy(key, ref, dim, step)
        copy.start()
        self.copies[key] = copy

    def recv(self, key, ref):
        self.copy(key, ref, "x", 1).wait_recv()

    def dim(self, c, stage):
        first = CLASSES[c][0]
        return first if stage == 1 else ("y" if first == "x" else "x")

    def hop_one(self, g, c, stage):
        own = self.piece(g, c, stage, 0)
        self.send((g, c, stage, "f1"), own, self.dim(c, stage), 1)
        self.send((g, c, stage, "b1"), own, self.dim(c, stage), -1)

    def hop_two(self, g, c, stage):
        d = self.dim(c, stage)
        self.recv((g, c, stage, "f1"), self.piece(g, c, stage, -1))
        self.send((g, c, stage, "f2"), self.piece(g, c, stage, -1, 0), d, 1)
        self.recv((g, c, stage, "b1"), self.piece(g, c, stage, 1))
        self.send((g, c, stage, "b2"), self.piece(g, c, stage, 1, 1), d, -1)

    def hop_end(self, g, c, stage):
        self.recv((g, c, stage, "f2"), self.piece(g, c, stage, 2, 0))
        self.recv((g, c, stage, "b2"), self.piece(g, c, stage, 2, 1))

    def zkey(self, g, c, stage, off):
        return (g, c, stage, "z", off)

    def zsend(self, g, c, stage, off):
        self.send(
            self.zkey(g, c, stage, off),
            self.piece(g, c, stage, off, z=self.l),
            "z",
            CLASSES[c][1],
        )

    def zrecv(self, g, c, stage, off):
        self.recv(
            self.zkey(g, c, stage, off), self.piece(g, c, stage, off, z=1 - self.l)
        )

    def step(self, g, s):
        if s == 0:
            for c in (0, 1):
                self.hop_one(g, c, 1)
            for c in (2, 3, 0, 1):
                self.zsend(g, c, 1, 0)
        elif s == 1:
            for c in (2, 3):
                self.zrecv(g, c, 1, 0)
                self.hop_one(g, c, 1)
        elif s in (2, 6):
            stage = 1 if s == 2 else 2
            for c in (0, 1):
                self.hop_two(g, c, stage)
                self.zsend(g, c, stage, -1)
                self.zsend(g, c, stage, 1)
        elif s in (3, 7):
            for c in (2, 3):
                self.hop_two(g, c, 1 if s == 3 else 2)
        elif s in (4, 8):
            stage = 1 if s == 4 else 2
            for c in (0, 1):
                self.hop_end(g, c, stage)
                if stage == 1:
                    self.hop_one(g, c, 2)
                self.zsend(g, c, stage, 2)
        elif s == 5:
            for c in (2, 3):
                self.hop_end(g, c, 1)
                self.hop_one(g, c, 2)
        elif s == 9:
            for c in (2, 3):
                self.hop_end(g, c, 2)
            for c in (0, 1):
                for stage, off in ((1, 0), (1, -1), (1, 1), (1, 2), (2, -1), (2, 1), (2, 2)):
                    self.zrecv(g, c, stage, off)

    def enter(self):
        barrier = pltpu.get_barrier_semaphore()
        for d in self.neighbours():
            pl.semaphore_signal(barrier, inc=1, device_id=d, device_id_type=MESH)
        pl.semaphore_wait(barrier, 7)

    def leave(self):
        for copy in self.copies.values():
            copy.wait_send()


ORDER = (
    [(0, 0), (0, 1), (0, 2), (0, 3), (0, 4), (0, 5), (1, 0), (0, 6), (1, 1), (0, 7), (0, 8)]
    + [(1, 2), (1, 3), (1, 4), (1, 5), (0, 9), (2, 0), (1, 6), (2, 1), (1, 7), (1, 8)]
    + [(2, 2), (2, 3), (2, 4), (2, 5), (1, 9), (2, 6), (2, 7), (2, 8), (2, 9)]
)


def gather_kernel(p_ref, full, send_sem, recv_sem, sem):
    g = Gather(full, send_sem, recv_sem)
    own = pltpu.make_async_copy(p_ref, full.at[g.l, g.y, g.x], sem)
    own.start()
    own.wait()
    g.enter()
    for a in ORDER:
        g.step(*a)
    g.leave()


def gather_weights(p):
    return pl.pallas_call(
        gather_kernel,
        out_shape=jax.ShapeDtypeStruct((2, 4, 4, 64, COLS), jnp.bfloat16),
        in_specs=[pl.BlockSpec(memory_space=pl.ANY)],
        out_specs=pl.BlockSpec(memory_space=pl.ANY),
        scratch_shapes=[
            pltpu.SemaphoreType.DMA((NSEM,)),
            pltpu.SemaphoreType.DMA((NSEM,)),
            pltpu.SemaphoreType.DMA,
        ],
        compiler_params=pltpu.CompilerParams(collective_id=0, has_side_effects=True),
        name="gather",
    )(p).reshape(2048, COLS)

KEY_DIM = 64
VALUE_DIM = 128
BLOCK = 64
SEQ_LEN = 256


norm_eps = 1e-06
fading_sharpness = 16.0


def side_by_side(arrays, axis, dim, along):
    both = jnp.concatenate(arrays, axis=along)
    out, at, done = (lax.all_gather(both, axis, axis=dim, tiled=True), 0, [])
    for a in arrays:
        done.append(lax.slice_in_dim(out, at, at + a.shape[along], axis=along))
        at += a.shape[along]
    return tuple(done)


def laid_out(parts, dim):
    parts = jnp.moveaxis(parts, 0, dim)
    dims = parts.shape
    return parts.reshape(*dims[:dim], dims[dim] * dims[dim + 1], *dims[dim + 2 :])


def sent_to_all(value, axis):
    devices = lax.axis_size(axis)
    return lax.all_to_all(
        jnp.broadcast_to(value[None], (devices, *value.shape)), axis, 0, 0, tiled=True
    )


def gathered_copies(value, axis, dim):
    return laid_out(sent_to_all(value, axis), dim)


def over_copies(value, axis):
    everything = sent_to_all(value, axis)
    return jnp.sum(everything.astype(jnp.float32), axis=0)


def split_up(value, dim, devices):
    before, after = (value.shape[:dim], value.shape[dim + 1 :])
    return jnp.moveaxis(value.reshape(*before, devices, -1, *after), dim, 0)


def summed_on_arrival(value, axis, dim):
    parts = split_up(value, dim, lax.axis_size(axis))
    arrived = lax.all_to_all(parts, axis, split_axis=0, concat_axis=0, tiled=True)
    return arrived.astype(jnp.float32).sum(axis=0)


def normalize(source, gain):
    widened = source.astype(jnp.float32)
    scaled = widened * lax.rsqrt(jnp.mean(widened * widened, axis=-1, keepdims=True) + norm_eps)
    return (scaled * gain.astype(jnp.float32)).astype(jnp.bfloat16)


def direction(queries, key_heads, value_heads, fading_exponent):
    sequences, length, head_count, key_depth = queries.shape
    value_depth = value_heads.shape[-1]
    block_count = length // BLOCK
    query_blocks = queries.reshape(sequences, block_count, BLOCK, head_count, key_depth)
    key_blocks = key_heads.reshape(sequences, block_count, BLOCK, head_count, key_depth)
    value_blocks = value_heads.reshape(sequences, block_count, BLOCK, head_count, value_depth)
    cumulative = jnp.cumsum(
        fading_exponent.reshape(sequences, block_count, BLOCK, head_count, key_depth), axis=2
    )
    block_total = cumulative[:, :, -1:]
    query_decayed = query_blocks * jnp.exp(cumulative)
    key_inverse = key_blocks * jnp.exp(-cumulative)
    key_carried = key_blocks * jnp.exp(block_total - cumulative)
    lower_mask = jnp.tril(jnp.ones((BLOCK, BLOCK), dtype=bool))
    scores = jnp.einsum("snihd,snjhd->snhij", query_decayed, key_inverse)
    scores = jnp.where(lower_mask, scores, 0.0)
    within_block = jnp.einsum("snhij,snjhv->snihv", scores, value_blocks)
    increments = jnp.einsum("snchd,snchv->nshdv", key_carried, value_blocks)
    carry_decay = jnp.moveaxis(jnp.exp(block_total[:, :, 0]), 1, 0)

    def advance(running, inputs):
        factor, update = inputs
        return (factor[..., None] * running + update, running)

    initial = jnp.zeros((sequences, head_count, key_depth, value_depth), jnp.float32)
    unused, previous = lax.scan(advance, initial, (carry_decay, increments))
    across_blocks = jnp.einsum("snchd,nshdv->snchv", query_decayed, previous)
    return (within_block + across_blocks).reshape(sequences, length, head_count, value_depth)


def mixer_heads(queries_raw, keys_raw, values_raw, gates_raw, fading_exponent, per_head_gain):
    row_count = queries_raw.shape[0]
    head_count = values_raw.shape[1] // VALUE_DIM
    key_shape = (row_count // SEQ_LEN, SEQ_LEN, head_count, KEY_DIM)
    value_shape = (row_count // SEQ_LEN, SEQ_LEN, head_count, VALUE_DIM)
    queries = queries_raw.astype(jnp.float32).reshape(key_shape) * KEY_DIM ** (-0.5)
    key_heads = keys_raw.astype(jnp.float32).reshape(key_shape)
    value_heads = values_raw.astype(jnp.float32).reshape(value_shape)
    decay_heads = fading_exponent.reshape(key_shape)
    forward = direction(queries, key_heads, value_heads, decay_heads)
    backward = direction(
        jnp.flip(queries, 1),
        jnp.flip(key_heads, 1),
        jnp.flip(value_heads, 1),
        jnp.flip(decay_heads, 1),
    )
    attention = forward + jnp.flip(backward, 1)
    scaled = attention * lax.rsqrt(
        jnp.mean(attention * attention, axis=-1, keepdims=True) + norm_eps
    )
    scaled = scaled * per_head_gain.astype(jnp.float32)
    merged = scaled.reshape(row_count, head_count * VALUE_DIM)
    return (merged * jax.nn.silu(gates_raw.astype(jnp.float32))).astype(jnp.bfloat16)


def depthwise(linear_out, gated_out, depthwise_taps, depthwise_bias):
    row_count, channels = linear_out.shape

    def smooth(source, taps, offset_bias):
        framed = source.astype(jnp.float32).reshape(row_count // SEQ_LEN, SEQ_LEN, channels)
        tap_count = taps.shape[0]
        leading_zero_fill = tap_count // 2
        padded = jnp.pad(
            framed, ((0, 0), (leading_zero_fill, tap_count - 1 - leading_zero_fill), (0, 0))
        )
        result = offset_bias.astype(jnp.float32)
        for shift_index in range(tap_count):
            result = result + padded[:, shift_index : shift_index + SEQ_LEN] * taps[
                shift_index
            ].astype(jnp.float32)
        return result

    linear_conv = smooth(linear_out, depthwise_taps[0], depthwise_bias[0])
    gate_conv = smooth(gated_out, depthwise_taps[1], depthwise_bias[1])
    return (linear_conv * jax.nn.silu(gate_conv)).astype(jnp.bfloat16).reshape(row_count, channels)


def fold_rows(source, weight_pieces):
    return tuple(
        (
            jnp.dot(source, weight_piece, preferred_element_type=jnp.float32)
            for weight_piece in weight_pieces
        )
    )


def emit_with(source, weight_piece):
    return jnp.dot(source, weight_piece, preferred_element_type=jnp.float32)


def emit_nt(source, weight_rows):
    return lax.dot_general(
        source, weight_rows, (((1,), (1,)), ((), ())), preferred_element_type=jnp.float32
    )


def local(
    tokens,
    first_norm_gain,
    query_projection_weight,
    key_projection_weight,
    value_projection_weight,
    output_gate_weight,
    decay_projection_weight,
    fading_shift_vector,
    added_fading_exponent,
    per_head_gain,
    mixer_result_matrix,
    second_norm_gain,
    up_linear_weight,
    up_gating_weight,
    depthwise_taps,
    depthwise_bias,
    down_projection_weight,
):
    whole_rows = lax.all_gather(tokens, "tp", axis=1, tiled=True)
    normed = normalize(whole_rows, first_norm_gain)
    full = gather_weights(
        jnp.concatenate(
            (
                query_projection_weight,
                key_projection_weight,
                value_projection_weight,
                output_gate_weight,
                decay_projection_weight,
                mixer_result_matrix.T,
                up_linear_weight,
                up_gating_weight,
                down_projection_weight.T,
            ),
            axis=1,
        )
    )
    projected = emit_with(normed, full[:, :1792])
    mapped_token_matrix = jnp.split(projected, (256, 512, 1024, 1536), axis=1)
    queries_raw = mapped_token_matrix[0].astype(jnp.bfloat16)
    keys_raw = mapped_token_matrix[1].astype(jnp.bfloat16)
    values_raw = mapped_token_matrix[2].astype(jnp.bfloat16)
    gates_raw = mapped_token_matrix[3].astype(jnp.bfloat16)
    fading_exponent = (
        jax.nn.log_sigmoid(mapped_token_matrix[4] + fading_shift_vector) / fading_sharpness
        + added_fading_exponent
    )
    mixed_heads = mixer_heads(
        queries_raw, keys_raw, values_raw, gates_raw, fading_exponent, per_head_gain
    )
    mixer_terms = emit_nt(mixed_heads, full[:, 1792:2304])
    feature_share = tokens.shape[1]
    summed = over_copies(mixer_terms.astype(jnp.bfloat16), "tp").astype(jnp.float32)
    full_after = (whole_rows.astype(jnp.float32) + summed).astype(jnp.bfloat16)
    after_mixer = lax.dynamic_slice_in_dim(
        full_after, lax.axis_index("tp") * feature_share, feature_share, 1
    )
    normed_two = normalize(full_after, second_norm_gain)
    upward = jnp.split(emit_with(normed_two, full[:, 2304:5376]), 2, axis=1)
    linear_out = upward[0].astype(jnp.bfloat16)
    gated_out = upward[1].astype(jnp.bfloat16)
    hidden = depthwise(linear_out, gated_out, depthwise_taps, depthwise_bias)
    channel_terms = emit_nt(hidden, full[:, 5376:])
    channel_part = summed_on_arrival(channel_terms.astype(jnp.bfloat16), "tp", 1)
    return (after_mixer.astype(jnp.float32) + channel_part).astype(jnp.bfloat16)


def solution(mesh):
    return jax.shard_map(
        local,
        mesh=mesh,
        in_specs=(
            P(("rep", "fs"), "tp"),
            P(),
            P("fs", "tp"),
            P("fs", "tp"),
            P("fs", "tp"),
            P("fs", "tp"),
            P("fs", "tp"),
            P("tp"),
            P(("rep", "fs"), "tp"),
            P(),
            P("tp", "fs"),
            P(),
            P("fs", "tp"),
            P("fs", "tp"),
            P(None, None, "tp"),
            P(None, "tp"),
            P("tp", "fs"),
        ),
        out_specs=P(("rep", "fs"), "tp"),
        check_vma=False,
    )
```

```python
import jax
import jax.numpy as jnp
from jax import lax
from jax.experimental import pallas as pl
from jax.experimental.pallas import tpu as pltpu
from jax.sharding import PartitionSpec as P

LANE = 128
MESH = pl.DeviceIdType.MESH
GROUPS = ((0, (6, 5, 3, 4)), (18, (7, 8, 5, 4)), (42, (4, 4, 2, 2)))
COLS = 54 * LANE
CLASSES = (("x", 1, True), ("y", -1, True), ("x", 1, False), ("y", -1, False))
NSEM = 144


class Gather:
    def __init__(self, full, send_sem, recv_sem):
        self.full, self.send_sem, self.recv_sem = full, send_sem, recv_sem
        rep, fs, self.tp = (lax.axis_index(a) for a in ("rep", "fs", "tp"))
        self.x, self.y, self.l = lax.rem(fs, 4), lax.rem(fs // 4, 4), fs // 16
        self.z = rep * 2 + self.l
        self.ids, self.sent = {}, {}

    def device(self, dim, step):
        x, y, z = self.x, self.y, self.z
        if dim == "x":
            x = lax.rem(x + step + 4, 4)
        elif dim == "y":
            y = lax.rem(y + step + 4, 4)
        else:
            z = lax.rem(z + step + 4, 4)
        return (z // 2, lax.rem(z, 2) * 16 + y * 4 + x, self.tp)

    def neighbours(self):
        return [self.device(d, s) for d in "xyz" for s in (1, -1)] + [
            (self.z // 2, self.l * 16 + self.y * 4 + self.x, 1 - self.tp)
        ]

    def cols(self, g, c):
        at, widths = GROUPS[g]
        return pl.ds((at + sum(widths[:c])) * LANE, widths[c] * LANE)

    def piece(self, g, c, stage, off, half=None, z=None):
        first, _, last = CLASSES[c]
        if z is None:
            zs = pl.ds(self.l, 1) if last else pl.ds(0, 2)
        else:
            zs = pl.ds(z, 1)
        rows = pl.ds(0, 64) if half is None else pl.ds(32 * half, 32)
        dim = first if stage == 1 else ("y" if first == "x" else "x")
        mine = self.x if dim == "x" else self.y
        at = pl.ds(lax.rem(mine + off + 4, 4), 1)
        if stage == 1:
            other = pl.ds(self.y if dim == "x" else self.x, 1)
        else:
            other = pl.ds(0, 4)
        yx = (other, at) if dim == "x" else (at, other)
        return self.full.at[zs, yx[0], yx[1], rows, self.cols(g, c)]

    def copy(self, key, ref, dim, step):
        i = self.ids.setdefault(key, len(self.ids))
        return pltpu.make_async_remote_copy(
            src_ref=ref,
            dst_ref=ref,
            send_sem=self.send_sem.at[i],
            recv_sem=self.recv_sem.at[i],
            device_id=self.device(dim, step),
            device_id_type=MESH,
        )

    def send(self, key, ref_args, dim, step):
        copy = self.copy(key, self.piece(*ref_args), dim, step)
        copy.start()
        self.sent[key] = (ref_args, dim, step)

    def recv(self, key, ref):
        self.copy(key, ref, "x", 1).wait_recv()

    def dim(self, c, stage):
        first = CLASSES[c][0]
        return first if stage == 1 else ("y" if first == "x" else "x")

    def hop_one(self, g, c, stage):
        own = (g, c, stage, 0)
        self.send((g, c, stage, "f1"), own, self.dim(c, stage), 1)
        self.send((g, c, stage, "b1"), own, self.dim(c, stage), -1)

    def hop_two(self, g, c, stage):
        d = self.dim(c, stage)
        self.recv((g, c, stage, "f1"), self.piece(g, c, stage, -1))
        self.send((g, c, stage, "f2"), (g, c, stage, -1, 0), d, 1)
        self.recv((g, c, stage, "b1"), self.piece(g, c, stage, 1))
        self.send((g, c, stage, "b2"), (g, c, stage, 1, 1), d, -1)

    def hop_end(self, g, c, stage):
        self.recv((g, c, stage, "f2"), self.piece(g, c, stage, 2, 0))
        self.recv((g, c, stage, "b2"), self.piece(g, c, stage, 2, 1))

    def zkey(self, g, c, stage, off):
        return (g, c, stage, "z", off)

    def zsend(self, g, c, stage, off):
        self.send(
            self.zkey(g, c, stage, off),
            (g, c, stage, off, None, self.l),
            "z",
            CLASSES[c][1],
        )

    def zrecv(self, g, c, stage, off):
        self.recv(
            self.zkey(g, c, stage, off), self.piece(g, c, stage, off, z=1 - self.l)
        )

    def step(self, g, s):
        if s == 0:
            for c in (0, 1):
                self.hop_one(g, c, 1)
            for c in (2, 3, 0, 1):
                self.zsend(g, c, 1, 0)
        elif s == 1:
            for c in (2, 3):
                self.zrecv(g, c, 1, 0)
                self.hop_one(g, c, 1)
        elif s in (2, 6):
            stage = 1 if s == 2 else 2
            for c in (0, 1):
                self.hop_two(g, c, stage)
                self.zsend(g, c, stage, -1)
                self.zsend(g, c, stage, 1)
        elif s in (3, 7):
            for c in (2, 3):
                self.hop_two(g, c, 1 if s == 3 else 2)
        elif s in (4, 8):
            stage = 1 if s == 4 else 2
            for c in (0, 1):
                self.hop_end(g, c, stage)
                if stage == 1:
                    self.hop_one(g, c, 2)
                self.zsend(g, c, stage, 2)
        elif s == 5:
            for c in (2, 3):
                self.hop_end(g, c, 1)
                self.hop_one(g, c, 2)
        elif s == 9:
            for c in (2, 3):
                self.hop_end(g, c, 2)
            for c in (0, 1):
                for stage, off in ((1, 0), (1, -1), (1, 1), (1, 2), (2, -1), (2, 1), (2, 2)):
                    self.zrecv(g, c, stage, off)

    def enter(self):
        barrier = pltpu.get_barrier_semaphore()
        for d in self.neighbours():
            pl.semaphore_signal(barrier, inc=1, device_id=d, device_id_type=MESH)
        pl.semaphore_wait(barrier, 7)

    def partner(self):
        return (self.z // 2, self.l * 16 + self.y * 4 + self.x, 1 - self.tp)

    def steps(self, todo):
        for g, s in todo:
            self.step(g, s)

    def steps_in(self, i, plan):
        for at, todo in plan.items():

            @pl.when(i == at)
            def _():
                self.steps(todo)

    def leave(self):
        for key, (ref_args, dim, step) in self.sent.items():
            self.copy(key, self.piece(*ref_args), dim, step).wait_send()


ROWS = 768
SEQ = 256
HALF = 1024
NORM_EPS = 1e-06
SHARPNESS = 16.0
MIX_AT, UP_AT, DOWN_AT, FF = 1792, 2304, 5376, 1536
ROW_STEP = 16
F32, BF16 = jnp.float32, jnp.bfloat16

PLAN = {
    "open": [(0, 0)],
    "tokens": [(0, 1)],
    "norm": {8: [(0, 2)], 16: [(0, 3)], 32: [(0, 4), (0, 5), (1, 0)]},
    "first": [(0, 6), (1, 1), (0, 7), (0, 8), (1, 2), (1, 3), (1, 4), (1, 5), (0, 9), (2, 0)],
    "project": {5: [(1, 6), (2, 1)]},
    "heads": {1: [(1, 7)], 3: [(2, 2)]},
    "mix": {1: [(1, 8), (2, 3)], 5: [(2, 4)]},
    "second": {0: [(2, 5)]},
    "up_first": [(1, 9)],
    "up": {1: [(2, 6)], 3: [(2, 7)], 4: [(2, 8)]},
    "last": [(2, 9)],
}


def dot(a, b):
    return jnp.dot(a, b, preferred_element_type=F32)


def dot_nt(a, b):
    return lax.dot_general(a, b, (((1,), (1,)), ((), ())), preferred_element_type=F32)


def normalize(parts, gain_ref):
    total = sum(jnp.sum(p * p, axis=-1, keepdims=True) for p in parts)
    scale = lax.rsqrt(total * (1.0 / 2048) + NORM_EPS)
    width = 2048 // len(parts)
    return [
        (p * scale * gain_ref[:, i * width : (i + 1) * width].astype(F32)).astype(BF16)
        for i, p in enumerate(parts)
    ]


def head_pair(s, pair, qkvg, decay, mixed, head_gain):
    rows = pl.ds(pl.multiple_of(s * SEQ, SEQ), SEQ)
    at = pl.multiple_of(pair * LANE, LANE)
    lane = lax.broadcasted_iota(jnp.int32, (1, LANE), 1)
    low = lane < 64
    t = lax.broadcasted_iota(jnp.int32, (SEQ, SEQ), 0)
    u = lax.broadcasted_iota(jnp.int32, (SEQ, SEQ), 1)
    before = u <= t
    after = u >= t

    log_a = decay[rows, pl.ds(at, LANE)]
    ones = before.astype(F32).astype(BF16)
    high = log_a.astype(BF16)
    rest = log_a - high.astype(F32)
    middle = rest.astype(BF16)
    small = (rest - middle.astype(F32)).astype(BF16)
    done = dot(ones, high) + (dot(ones, middle) + dot(ones, small))
    open_ = done - log_a
    mid = [done[64 * b + 31 : 64 * b + 32] for b in range(4)]
    mid_open = [open_[64 * b + 32 : 64 * b + 33] for b in range(4)]

    q = qkvg[rows, pl.ds(at, LANE)].astype(F32) * 0.125
    k = qkvg[rows, pl.ds(pl.multiple_of(at + 256, LANE), LANE)].astype(F32)
    blocks = [slice(64 * b, 64 * b + 64) for b in range(4)]
    key_fwd = [k[r] * jnp.exp(mid[b] - done[r]) for b, r in enumerate(blocks)]
    key_bwd = [k[r] * jnp.exp(open_[r] - mid_open[b]) for b, r in enumerate(blocks)]

    def swap(v):
        return pltpu.roll(v, 64, 1)

    def both(v, parity):
        other = swap(v)
        return jnp.where(low, v, other) if parity == 0 else jnp.where(low, other, v)

    nothing = jnp.zeros((64, LANE), BF16)

    def side(queries, points, mids, keys, backward, parity):
        sign = -1.0 if backward else 1.0
        point_mids = [
            jnp.where(low, both(mids[2 * p], parity), both(mids[2 * p + 1], parity))
            for p in range(2)
        ]
        left, right = [], []
        for b, r in enumerate(blocks):
            row = []
            for p in range(2):
                expo = (points[r] - point_mids[p]) * sign
                if backward:
                    used = (b <= 2 * p, b <= 2 * p + 1)
                else:
                    used = (b >= 2 * p, b >= 2 * p + 1)
                if not any(used):
                    row.append(nothing)
                    continue
                if not all(used):
                    expo = jnp.where(low if used[0] else ~low, expo, -1e30)
                row.append((queries[r] * jnp.exp(expo)).astype(BF16))
            left.append(jnp.concatenate(row, axis=1))
            mine = keys[b] if parity == b % 2 else swap(keys[b])
            mine = jnp.where(low if b % 2 == 0 else ~low, mine, 0.0).astype(BF16)
            right.append(
                jnp.concatenate([mine if p == b // 2 else nothing for p in range(2)], axis=1)
            )
        return dot_nt(jnp.concatenate(left, axis=0), jnp.concatenate(right, axis=0))

    for parity in range(2):
        queries = both(q, parity)
        fwd = side(queries, both(done, parity), mid, key_fwd, False, parity)
        bwd = side(queries, both(open_, parity), mid_open, key_bwd, True, parity)
        scores = jnp.where(before, fwd, 0.0) + jnp.where(after, bwd, 0.0)
        place = pl.multiple_of(pair * 256 + parity * LANE, LANE)
        values = qkvg[rows, pl.ds(pl.multiple_of(place + 512, LANE), LANE)]
        out = dot(scores.astype(BF16), values)
        scale = lax.rsqrt(jnp.mean(out * out, axis=-1, keepdims=True) + NORM_EPS)
        out = out * scale * head_gain[...].astype(F32)
        gate = qkvg[rows, pl.ds(pl.multiple_of(place + 1024, LANE), LANE)].astype(F32)
        out = out * (gate * jax.nn.sigmoid(gate))
        mixed[rows, pl.ds(place, LANE)] = out.astype(BF16)


def smooth(source, taps, bias):
    row = lax.broadcasted_iota(jnp.int32, source.shape, 0)
    back = jnp.where(row == 0, 0.0, pltpu.roll(source, 1, 0))
    ahead = jnp.where(row == SEQ - 1, 0.0, pltpu.roll(source, SEQ - 1, 0))
    return bias + back * taps[0:1] + source * taps[1:2] + ahead * taps[2:3]


def layer_kernel(
    tokens,
    wq,
    wk,
    wv,
    wg,
    wd,
    mix_t,
    up_lin,
    up_gate,
    down_t,
    added,
    gain_one,
    shift,
    head_gain,
    gain_two,
    taps,
    bias,
    out,
    full,
    tok,
    normed,
    qkvg,
    decay,
    fading,
    mixed,
    mix_out,
    mix_in,
    hidden,
    down_out,
    down_in,
    result,
    send_sem,
    recv_sem,
    load_sem,
    pair_send,
    pair_recv,
    out_sem,
):
    g = Gather(full, send_sem, recv_sem)
    tp = g.tp
    own = full.at[g.l, g.y, g.x]
    loads = [pltpu.make_async_copy(tokens, tok.at[tp], load_sem.at[0])]
    at = 0
    for n, w in enumerate((wq, wk, wv, wg, wd, mix_t, up_lin, up_gate, down_t)):
        width = w.shape[1]
        loads.append(
            pltpu.make_async_copy(w, own.at[:, pl.ds(at, width)], load_sem.at[n + 1])
        )
        at += width
    fading_load = pltpu.make_async_copy(added, fading, load_sem.at[10])
    for load in loads:
        load.start()
    fading_load.start()
    g.enter()

    def to_partner(src, dst, n):
        return pltpu.make_async_remote_copy(
            src_ref=src,
            dst_ref=dst,
            send_sem=pair_send.at[n],
            recv_sem=pair_recv.at[n],
            device_id=g.partner(),
            device_id_type=MESH,
        )

    for load in loads[1:7]:
        load.wait()
    for load in loads[7:]:
        load.wait()
    g.steps(PLAN["open"])
    loads[0].wait()
    swap_tokens = to_partner(tok.at[tp], tok.at[tp], 0)
    swap_tokens.start()
    fading_load.wait()
    g.steps(PLAN["tokens"])
    to_partner(tok.at[tp], tok.at[1 - tp], 0).wait_recv()

    def first_norm(i, _):
        rows = pl.ds(pl.multiple_of(i * ROW_STEP, ROW_STEP), ROW_STEP)
        parts = normalize([tok[h, rows, :].astype(F32) for h in range(2)], gain_one)
        for h in range(2):
            normed[rows, h * HALF : (h + 1) * HALF] = parts[h]
        g.steps_in(i, PLAN["norm"])
        return 0

    lax.fori_loop(0, ROWS // ROW_STEP, first_norm, 0)
    g.steps(PLAN["first"])

    score = dot(normed[...], full[:, :, :, :, 1536:1792].reshape(2048, 256)) + shift[...]
    faded = jnp.minimum(score, 0.0) - jnp.log1p(jnp.exp(-jnp.abs(score)))
    decay[...] = faded * (1.0 / SHARPNESS) + fading[...]

    def project(j, _):
        cols = pl.ds(pl.multiple_of(j * 256, 256), 256)
        weight = full[:, :, :, :, cols].reshape(2048, 256)
        qkvg[:, cols] = dot(normed[...], weight).astype(BF16)
        g.steps_in(j, PLAN["project"])
        return 0

    lax.fori_loop(0, 6, project, 0)

    def heads(i, _):
        head_pair(i // 2, lax.rem(i, 2), qkvg, decay, mixed, head_gain)
        g.steps_in(i, PLAN["heads"])
        return 0

    lax.fori_loop(0, 6, heads, 0)

    def mix(j, _):
        weight = full[j // 4, lax.rem(j, 4), :, :, MIX_AT:UP_AT].reshape(256, 512)
        mix_out[j] = dot_nt(mixed[...], weight).astype(BF16)
        to_partner(mix_out.at[j], mix_in.at[j], 1 + j).start()
        g.steps_in(j, PLAN["mix"])
        return 0

    lax.fori_loop(0, 8, mix, 0)
    for j in range(8):
        to_partner(mix_out.at[j], mix_in.at[j], 1 + j).wait_recv()

    def second_norm(i, _):
        rows = pl.ds(pl.multiple_of(i * ROW_STEP, ROW_STEP), ROW_STEP)
        parts = []
        for j in range(8):
            cols = slice((j % 4) * 256, (j % 4 + 1) * 256)
            term = mix_out[j, rows, :].astype(F32) + mix_in[j, rows, :].astype(F32)
            kept = (tok[j // 4, rows, cols].astype(F32) + term).astype(BF16)
            tok[j // 4, rows, cols] = kept
            parts.append(kept.astype(F32))
        for j, part in enumerate(normalize(parts, gain_two)):
            normed[rows, j * 256 : (j + 1) * 256] = part
        g.steps_in(i, PLAN["second"])
        return 0

    swap_tokens.wait_send()
    lax.fori_loop(0, ROWS // ROW_STEP, second_norm, 0)
    g.steps(PLAN["up_first"])

    def up(j, _):
        cols = pl.ds(pl.multiple_of(j * 256, 256), 256)
        parts = []
        for half in range(2):
            at = pl.multiple_of(UP_AT + half * FF + j * 256, 256)
            weight = full[:, :, :, :, pl.ds(at, 256)].reshape(2048, 256)
            parts.append(dot(normed[...], weight).astype(BF16))
        tap = [taps[half, :, cols].astype(F32) for half in range(2)]
        base = bias[:, cols].astype(F32)
        for s in range(ROWS // SEQ):
            rows = slice(s * SEQ, (s + 1) * SEQ)
            lin, gate = (
                smooth(parts[h][rows].astype(F32), tap[h], base[h : h + 1]) for h in range(2)
            )
            hidden[rows, cols] = (lin * (gate * jax.nn.sigmoid(gate))).astype(BF16)
        g.steps_in(j, PLAN["up"])
        return 0

    lax.fori_loop(0, FF // 256, up, 0)
    g.steps(PLAN["last"])

    def down_part(half, j):
        weight = full[half, j, :, :, DOWN_AT:COLS].reshape(256, FF)
        return dot_nt(hidden[...], weight).astype(BF16)

    def down_theirs(j, _):
        down_out[j] = down_part(1 - tp, j)
        to_partner(down_out.at[j], down_in.at[j], 9 + j).start()
        return 0

    lax.fori_loop(0, 4, down_theirs, 0)

    def stored(j):
        return pltpu.make_async_copy(
            result.at[j],
            out.at[:, pl.ds(pl.multiple_of(j * 256, 256), 256)],
            out_sem.at[j],
        )

    def down_mine(j, _):
        mine = down_part(tp, j).astype(F32)
        to_partner(down_out.at[j], down_in.at[j], 9 + j).wait_recv()
        cols = pl.ds(pl.multiple_of(j * 256, 256), 256)
        summed = mine + down_in[j].astype(F32)
        result[j] = (tok[tp, :, cols].astype(F32) + summed).astype(BF16)
        stored(j).start()
        return 0

    lax.fori_loop(0, 4, down_mine, 0)
    for j in range(8):
        to_partner(mix_out.at[j], mix_in.at[j], 1 + j).wait_send()
    for j in range(4):
        to_partner(down_out.at[j], down_in.at[j], 9 + j).wait_send()
        stored(j).wait()
    g.leave()


def local(
    tokens,
    first_norm_gain,
    query_projection_weight,
    key_projection_weight,
    value_projection_weight,
    output_gate_weight,
    decay_projection_weight,
    fading_shift_vector,
    added_fading_exponent,
    per_head_gain,
    mixer_result_matrix,
    second_norm_gain,
    up_linear_weight,
    up_gating_weight,
    depthwise_taps,
    depthwise_bias,
    down_projection_weight,
):
    any_spec = pl.BlockSpec(memory_space=pl.ANY)
    vmem_spec = pl.BlockSpec(memory_space=pltpu.VMEM)
    dma = pltpu.SemaphoreType.DMA
    return pl.pallas_call(
        layer_kernel,
        out_shape=jax.ShapeDtypeStruct((ROWS, HALF), BF16),
        in_specs=[any_spec] * 11 + [vmem_spec] * 6,
        out_specs=any_spec,
        scratch_shapes=[
            pltpu.VMEM((2, 4, 4, 64, COLS), BF16),
            pltpu.VMEM((2, ROWS, HALF), BF16),
            pltpu.VMEM((ROWS, 2048), BF16),
            pltpu.VMEM((ROWS, 1536), BF16),
            pltpu.VMEM((ROWS, 256), F32),
            pltpu.VMEM((ROWS, 256), F32),
            pltpu.VMEM((ROWS, 512), BF16),
            pltpu.VMEM((8, ROWS, 256), BF16),
            pltpu.VMEM((8, ROWS, 256), BF16),
            pltpu.VMEM((ROWS, FF), BF16),
            pltpu.VMEM((4, ROWS, 256), BF16),
            pltpu.VMEM((4, ROWS, 256), BF16),
            pltpu.VMEM((4, ROWS, 256), BF16),
            dma((NSEM,)),
            dma((NSEM,)),
            dma((11,)),
            dma((13,)),
            dma((13,)),
            dma((4,)),
        ],
        compiler_params=pltpu.CompilerParams(
            collective_id=0, has_side_effects=True, vmem_limit_bytes=67043328
        ),
        name="layer",
    )(
        tokens,
        query_projection_weight,
        key_projection_weight,
        value_projection_weight,
        output_gate_weight,
        decay_projection_weight,
        mixer_result_matrix.T,
        up_linear_weight,
        up_gating_weight,
        down_projection_weight.T,
        added_fading_exponent,
        first_norm_gain[None],
        fading_shift_vector[None],
        per_head_gain[None],
        second_norm_gain[None],
        depthwise_taps,
        depthwise_bias,
    )


def solution(mesh):
    return jax.shard_map(
        local,
        mesh=mesh,
        in_specs=(
            P(("rep", "fs"), "tp"),
            P(),
            P("fs", "tp"),
            P("fs", "tp"),
            P("fs", "tp"),
            P("fs", "tp"),
            P("fs", "tp"),
            P("tp"),
            P(("rep", "fs"), "tp"),
            P(),
            P("tp", "fs"),
            P(),
            P("fs", "tp"),
            P("fs", "tp"),
            P(None, None, "tp"),
            P(None, "tp"),
            P("tp", "fs"),
        ),
        out_specs=P(("rep", "fs"), "tp"),
        check_vma=False,
    )
```

```python
import jax
import jax.numpy as jnp
from jax import lax
from jax.experimental import pallas as pl
from jax.experimental.pallas import tpu as pltpu
from jax.sharding import PartitionSpec as P

LANE = 128
MESH = pl.DeviceIdType.MESH
GROUPS = ((0, (5, 6, 4, 3)), (18, (8, 7, 4, 5)), (42, (3, 3, 3, 3)))
COLS = 54 * LANE
CLASSES = (("x", 1, True), ("y", -1, True), ("x", 1, False), ("y", -1, False))
NSEM = 144


class Gather:
    def __init__(self, full, send_sem, recv_sem):
        self.full, self.send_sem, self.recv_sem = full, send_sem, recv_sem
        rep, fs, self.tp = (lax.axis_index(a) for a in ("rep", "fs", "tp"))
        self.x, self.y, self.l = lax.rem(fs, 4), lax.rem(fs // 4, 4), fs // 16
        self.z = rep * 2 + self.l
        self.ids, self.sent = {}, {}

    def device(self, dim, step):
        x, y, z = self.x, self.y, self.z
        if dim == "x":
            x = lax.rem(x + step + 4, 4)
        elif dim == "y":
            y = lax.rem(y + step + 4, 4)
        else:
            z = lax.rem(z + step + 4, 4)
        return (z // 2, lax.rem(z, 2) * 16 + y * 4 + x, self.tp)

    def neighbours(self):
        return [self.device(d, s) for d in "xyz" for s in (1, -1)] + [
            (self.z // 2, self.l * 16 + self.y * 4 + self.x, 1 - self.tp)
        ]

    def cols(self, g, c):
        at, widths = GROUPS[g]
        return pl.ds((at + sum(widths[:c])) * LANE, widths[c] * LANE)

    def piece(self, g, c, stage, off, half=None, z=None):
        first, _, last = CLASSES[c]
        if z is None:
            zs = pl.ds(self.l, 1) if last else pl.ds(0, 2)
        else:
            zs = pl.ds(z, 1)
        rows = pl.ds(0, 64) if half is None else pl.ds(32 * half, 32)
        dim = first if stage == 1 else ("y" if first == "x" else "x")
        mine = self.x if dim == "x" else self.y
        at = pl.ds(lax.rem(mine + off + 4, 4), 1)
        if stage == 1:
            other = pl.ds(self.y if dim == "x" else self.x, 1)
        else:
            other = pl.ds(0, 4)
        yx = (other, at) if dim == "x" else (at, other)
        return self.full.at[zs, yx[0], yx[1], rows, self.cols(g, c)]

    def copy(self, key, ref, dim, step):
        i = self.ids.setdefault(key, len(self.ids))
        return pltpu.make_async_remote_copy(
            src_ref=ref,
            dst_ref=ref,
            send_sem=self.send_sem.at[i],
            recv_sem=self.recv_sem.at[i],
            device_id=self.device(dim, step),
            device_id_type=MESH,
        )

    def send(self, key, ref_args, dim, step):
        copy = self.copy(key, self.piece(*ref_args), dim, step)
        copy.start()
        self.sent[key] = (ref_args, dim, step)

    def recv(self, key, ref):
        self.copy(key, ref, "x", 1).wait_recv()

    def dim(self, c, stage):
        first = CLASSES[c][0]
        return first if stage == 1 else ("y" if first == "x" else "x")

    def hop_one(self, g, c, stage):
        own = (g, c, stage, 0)
        self.send((g, c, stage, "f1"), own, self.dim(c, stage), 1)
        self.send((g, c, stage, "b1"), own, self.dim(c, stage), -1)

    def hop_two(self, g, c, stage):
        d = self.dim(c, stage)
        self.recv((g, c, stage, "f1"), self.piece(g, c, stage, -1))
        self.send((g, c, stage, "f2"), (g, c, stage, -1, 0), d, 1)
        self.recv((g, c, stage, "b1"), self.piece(g, c, stage, 1))
        self.send((g, c, stage, "b2"), (g, c, stage, 1, 1), d, -1)

    def hop_end(self, g, c, stage):
        self.recv((g, c, stage, "f2"), self.piece(g, c, stage, 2, 0))
        self.recv((g, c, stage, "b2"), self.piece(g, c, stage, 2, 1))

    def zkey(self, g, c, stage, off):
        return (g, c, stage, "z", off)

    def zsend(self, g, c, stage, off):
        self.send(
            self.zkey(g, c, stage, off),
            (g, c, stage, off, None, self.l),
            "z",
            CLASSES[c][1],
        )

    def zrecv(self, g, c, stage, off):
        self.recv(
            self.zkey(g, c, stage, off), self.piece(g, c, stage, off, z=1 - self.l)
        )

    def unit(self, g, c, k):
        last = CLASSES[c][2]
        if k == 0:
            if last:
                self.hop_one(g, c, 1)
            self.zsend(g, c, 1, 0)
        elif k == 1:
            self.zrecv(g, c, 1, 0)
            self.hop_one(g, c, 1)
        elif k in (2, 3, 6, 7):
            stage = 1 if k < 4 else 2
            self.hop_two(g, c, stage)
            if last:
                self.zsend(g, c, stage, -1)
                self.zsend(g, c, stage, 1)
        elif k in (4, 5):
            self.hop_end(g, c, 1)
            self.hop_one(g, c, 2)
            if last:
                self.zsend(g, c, 1, 2)
        elif k == 8:
            self.hop_end(g, c, 2)
            self.zsend(g, c, 2, 2)

    def gathered(self, g):
        for c in (2, 3):
            self.hop_end(g, c, 2)
        for c in (0, 1):
            for off in (0, -1, 1, 2):
                self.zrecv(g, c, 1, off)
            for off in (-1, 1, 2):
                self.zrecv(g, c, 2, off)

    def enter(self):
        barrier = pltpu.get_barrier_semaphore()
        for d in self.neighbours():
            pl.semaphore_signal(barrier, inc=1, device_id=d, device_id_type=MESH)
        pl.semaphore_wait(barrier, 7)

    def partner(self):
        return (self.z // 2, self.l * 16 + self.y * 4 + self.x, 1 - self.tp)

    def steps(self, phase, i=0):
        for todo in PLAN.get(phase, {}).get(i, ()):
            self.unit(*todo)

    def steps_in(self, i, phase, every=1, start=0):
        for at in sorted(set(PLAN.get(phase, {})) - set(range(start))):

            @pl.when(i == at * every + every - 1)
            def _():
                self.steps(phase, at)

    def leave(self):
        for key, (ref_args, dim, step) in self.sent.items():
            self.copy(key, self.piece(*ref_args), dim, step).wait_send()


LIMIT = 58720256
ROWS = 768
SEQ = 256
HALF = 1024
NORM_EPS = 1e-06
VALUE_DIM = 128
SHARPNESS = 16.0
MIX_AT, UP_AT, DOWN_AT, FF = 1792, 2304, 5376, 1536
ROW_STEP = 64
PER_UNIT = ROWS // ROW_STEP // 6
F32, BF16 = jnp.float32, jnp.bfloat16

PLAN = {
    'open': {
        0: [(2, 1, 0), (0, 3, 0), (0, 1, 0), (0, 2, 0), (0, 0, 0), (2, 3, 0)],
    },
    'norm': {
        0: [(1, 1, 0), (1, 0, 0), (0, 0, 2), (1, 2, 0), (0, 1, 2), (0, 3, 1), (0, 2, 1), (1, 0, 2), (2, 0, 0), (1, 1, 2), (0, 0, 4), (2, 2, 0), (0, 1, 4), (1, 3, 0), (0, 2, 3)],
        1: [(0, 3, 3), (2, 3, 1), (0, 0, 6), (1, 0, 4), (1, 1, 4), (0, 0, 8), (2, 0, 2), (0, 1, 6), (2, 2, 1), (1, 3, 1), (1, 2, 1), (0, 1, 8)],
        2: [(0, 2, 5), (2, 2, 3)],
        3: [(2, 3, 3), (0, 3, 5), (1, 1, 6)],
        4: [(1, 3, 3), (0, 2, 7), (1, 0, 6), (0, 3, 7), (2, 1, 2), (1, 1, 8), (1, 2, 3), (1, 3, 5)],
    },
    'project': {
        0: [(1, 2, 5)],
        4: [(2, 1, 4), (1, 0, 8)],
    },
    'heads': {
        4: [(2, 0, 4)],
    },
    'mix': {
        2: [(1, 3, 7)],
        6: [(1, 2, 7)],
    },
    'mixed': {
        0: [(2, 1, 6), (2, 0, 6)],
    },
    'second': {
        4: [(2, 2, 5), (2, 3, 5)],
    },
    'up': {
        2: [(2, 1, 8)],
        3: [(2, 2, 7), (2, 0, 8), (2, 3, 7)],
    },
}


def dot(a, b):
    return jnp.dot(a, b, preferred_element_type=F32)


def dot_nt(a, b):
    return lax.dot_general(a, b, (((1,), (1,)), ((), ())), preferred_element_type=F32)


def normalize(parts, gain_ref):
    total = sum(jnp.sum(p * p, axis=-1, keepdims=True) for p in parts)
    scale = lax.rsqrt(total * (1.0 / 2048) + NORM_EPS)
    width = 2048 // len(parts)
    return [
        (p * scale * gain_ref[:, i * width : (i + 1) * width]).astype(BF16)
        for i, p in enumerate(parts)
    ]


def head_pair(s, pair, qkvg, decay, mixed, head_gain):
    rows = pl.ds(pl.multiple_of(s * SEQ, SEQ), SEQ)
    at = pl.multiple_of(pair * LANE, LANE)
    lane = lax.broadcasted_iota(jnp.int32, (1, LANE), 1)
    low = lane < 64
    t = lax.broadcasted_iota(jnp.int32, (SEQ, SEQ), 0)
    u = lax.broadcasted_iota(jnp.int32, (SEQ, SEQ), 1)
    before = u <= t
    after = u >= t

    log_a = decay[rows, pl.ds(at, LANE)]
    ones = before.astype(F32).astype(BF16)
    high = log_a.astype(BF16)
    rest = log_a - high.astype(F32)
    middle = rest.astype(BF16)
    small = (rest - middle.astype(F32)).astype(BF16)
    done = dot(ones, high) + (dot(ones, middle) + dot(ones, small))
    open_ = done - log_a
    mid = [done[64 * b + 31 : 64 * b + 32] for b in range(4)]
    mid_open = [open_[64 * b + 32 : 64 * b + 33] for b in range(4)]

    q = qkvg[rows, pl.ds(at, LANE)].astype(F32) * 0.125
    k = qkvg[rows, pl.ds(pl.multiple_of(at + 256, LANE), LANE)].astype(F32)
    blocks = [slice(64 * b, 64 * b + 64) for b in range(4)]
    key_fwd = [k[r] * jnp.exp(mid[b] - done[r]) for b, r in enumerate(blocks)]
    key_bwd = [k[r] * jnp.exp(open_[r] - mid_open[b]) for b, r in enumerate(blocks)]

    def swap(v):
        return pltpu.roll(v, 64, 1)

    def both(v, parity):
        other = swap(v)
        return jnp.where(low, v, other) if parity == 0 else jnp.where(low, other, v)

    nothing = jnp.zeros((64, LANE), BF16)

    def side(queries, points, mids, keys, backward, parity):
        sign = -1.0 if backward else 1.0
        point_mids = [
            jnp.where(low, both(mids[2 * p], parity), both(mids[2 * p + 1], parity))
            for p in range(2)
        ]
        left, right = [], []
        for b, r in enumerate(blocks):
            row = []
            for p in range(2):
                expo = (points[r] - point_mids[p]) * sign
                if backward:
                    used = (b <= 2 * p, b <= 2 * p + 1)
                else:
                    used = (b >= 2 * p, b >= 2 * p + 1)
                if not any(used):
                    row.append(nothing)
                    continue
                if not all(used):
                    expo = jnp.where(low if used[0] else ~low, expo, -1e30)
                row.append((queries[r] * jnp.exp(expo)).astype(BF16))
            left.append(jnp.concatenate(row, axis=1))
            mine = keys[b] if parity == b % 2 else swap(keys[b])
            mine = jnp.where(low if b % 2 == 0 else ~low, mine, 0.0).astype(BF16)
            right.append(
                jnp.concatenate([mine if p == b // 2 else nothing for p in range(2)], axis=1)
            )
        return dot_nt(jnp.concatenate(left, axis=0), jnp.concatenate(right, axis=0))

    for parity in range(2):
        queries = both(q, parity)
        fwd = side(queries, both(done, parity), mid, key_fwd, False, parity)
        bwd = side(queries, both(open_, parity), mid_open, key_bwd, True, parity)
        scores = jnp.where(before, fwd, 0.0) + jnp.where(after, bwd, 0.0)
        place = pl.multiple_of(pair * 256 + parity * LANE, LANE)
        values = qkvg[rows, pl.ds(pl.multiple_of(place + 512, LANE), LANE)]
        out = dot(scores.astype(BF16), values)
        scale = lax.rsqrt(jnp.mean(out * out, axis=-1, keepdims=True) + NORM_EPS)
        out = out * scale * head_gain[...]
        gate = qkvg[rows, pl.ds(pl.multiple_of(place + 1024, LANE), LANE)].astype(F32)
        out = out * (gate * jax.nn.sigmoid(gate))
        mixed[rows, pl.ds(place, LANE)] = out.astype(BF16)


def smooth(source, taps, bias):
    row = lax.broadcasted_iota(jnp.int32, source.shape, 0)
    back = jnp.where(row == 0, 0.0, pltpu.roll(source, 1, 0))
    ahead = jnp.where(row == SEQ - 1, 0.0, pltpu.roll(source, SEQ - 1, 0))
    return bias + back * taps[0:1] + source * taps[1:2] + ahead * taps[2:3]


def layer_kernel(
    tokens,
    wq,
    wk,
    wv,
    wg,
    wd,
    mix_t,
    up_lin,
    up_gate,
    down_t,
    added,
    gain_one,
    shift,
    head_gain,
    gain_two,
    taps,
    bias,
    out,
    full,
    gains,
    tok,
    normed,
    qkvg,
    decay,
    fading,
    mixed,
    mix_out,
    mix_in,
    hidden,
    down_out,
    down_in,
    send_sem,
    recv_sem,
    load_sem,
    pair_send,
    pair_recv,
):
    g = Gather(full, send_sem, recv_sem)
    tp = g.tp
    gains[0:1] = gain_one[...].astype(F32)[None]
    gains[1:2] = gain_two[...].astype(F32)[None]
    gains[2:3, :VALUE_DIM] = head_gain[...].astype(F32)[None]
    gain_one, gain_two = gains.at[0:1], gains.at[1:2]
    head_gain = gains.at[2:3, :VALUE_DIM]
    own = full.at[g.l, g.y, g.x]
    loads = [pltpu.make_async_copy(tokens, tok.at[tp], load_sem.at[0])]
    at = 0
    for n, w in enumerate((wq, wk, wv, wg, wd, mix_t, up_lin, up_gate, down_t)):
        width = w.shape[1]
        loads.append(
            pltpu.make_async_copy(w, own.at[:, pl.ds(at, width)], load_sem.at[n + 1])
        )
        at += width
    fading_load = pltpu.make_async_copy(added, fading, load_sem.at[10])
    for load in loads:
        load.start()
    fading_load.start()
    g.enter()

    def to_partner(src, dst, n):
        return pltpu.make_async_remote_copy(
            src_ref=src,
            dst_ref=dst,
            send_sem=pair_send.at[n],
            recv_sem=pair_recv.at[n],
            device_id=g.partner(),
            device_id_type=MESH,
        )

    for load in loads[1:]:
        load.wait()
    g.steps("open")
    loads[0].wait()
    swap_tokens = to_partner(tok.at[tp], tok.at[tp], 0)
    swap_tokens.start()
    fading_load.wait()
    to_partner(tok.at[tp], tok.at[1 - tp], 0).wait_recv()

    def first_norm(i, _):
        rows = pl.ds(pl.multiple_of(i * ROW_STEP, ROW_STEP), ROW_STEP)
        parts = normalize([tok[h, rows, :].astype(F32) for h in range(2)], gain_one)
        for h in range(2):
            normed[rows, h * HALF : (h + 1) * HALF] = parts[h]
        g.steps_in(i, "norm", PER_UNIT)
        return 0

    lax.fori_loop(0, ROWS // ROW_STEP, first_norm, 0)
    g.gathered(0)
    g.steps("got0")

    score = dot(normed[...], full[:, :, :, :, 1536:1792].reshape(2048, 256)) + shift[...]
    faded = jnp.minimum(score, 0.0) - jnp.log1p(jnp.exp(-jnp.abs(score)))
    decay[...] = faded * (1.0 / SHARPNESS) + fading[...]

    g.steps("project")

    def project(j, _):
        cols = pl.ds(pl.multiple_of(j * 256, 256), 256)
        weight = full[:, :, :, :, cols].reshape(2048, 256)
        qkvg[:, cols] = dot(normed[...], weight).astype(BF16)
        g.steps_in(j + 1, "project", 1, 1)
        return 0

    lax.fori_loop(0, 6, project, 0)

    def heads(i, _):
        head_pair(i // 2, lax.rem(i, 2), qkvg, decay, mixed, head_gain)
        g.steps_in(i, "heads")
        return 0

    lax.fori_loop(0, 6, heads, 0)

    def mix(j, _):
        weight = full[j // 4, lax.rem(j, 4), :, :, MIX_AT:UP_AT].reshape(256, 512)
        mix_out[j] = dot_nt(mixed[...], weight).astype(BF16)
        to_partner(mix_out.at[j], mix_in.at[j], 1 + j).start()
        g.steps_in(j, "mix")
        return 0

    lax.fori_loop(0, 8, mix, 0)
    for j in range(8):
        to_partner(mix_out.at[j], mix_in.at[j], 1 + j).wait_recv()
    g.steps("mixed")

    def second_norm(i, _):
        rows = pl.ds(pl.multiple_of(i * ROW_STEP, ROW_STEP), ROW_STEP)
        parts = []
        for j in range(8):
            cols = slice((j % 4) * 256, (j % 4 + 1) * 256)
            term = mix_out[j, rows, :].astype(F32) + mix_in[j, rows, :].astype(F32)
            kept = (tok[j // 4, rows, cols].astype(F32) + term).astype(BF16)
            tok[j // 4, rows, cols] = kept
            parts.append(kept.astype(F32))
        for j, part in enumerate(normalize(parts, gain_two)):
            normed[rows, j * 256 : (j + 1) * 256] = part
        g.steps_in(i, "second", PER_UNIT)
        return 0

    swap_tokens.wait_send()
    lax.fori_loop(0, ROWS // ROW_STEP, second_norm, 0)
    g.gathered(1)
    g.steps("got1")

    def up(j, _):
        cols = pl.ds(pl.multiple_of(j * 256, 256), 256)
        parts = []
        for half in range(2):
            at = pl.multiple_of(UP_AT + half * FF + j * 256, 256)
            weight = full[:, :, :, :, pl.ds(at, 256)].reshape(2048, 256)
            parts.append(dot(normed[...], weight).astype(BF16))
        tap = [taps[:, half, cols].astype(F32) for half in range(2)]
        base = bias[:, cols].astype(F32)
        for s in range(ROWS // SEQ):
            rows = slice(s * SEQ, (s + 1) * SEQ)
            lin, gate = (
                smooth(parts[h][rows].astype(F32), tap[h], base[h : h + 1]) for h in range(2)
            )
            hidden[rows, cols] = (lin * (gate * jax.nn.sigmoid(gate))).astype(BF16)
        g.steps_in(j, "up")
        return 0

    lax.fori_loop(0, FF // 256, up, 0)
    g.gathered(2)

    def down_part(half, j):
        weight = full[half, j, :, :, DOWN_AT:COLS].reshape(256, FF)
        return dot_nt(hidden[...], weight).astype(BF16)

    def down_theirs(j, _):
        down_out[j] = down_part(1 - tp, j)
        to_partner(down_out.at[j], down_in.at[j], 9 + j).start()
        return 0

    lax.fori_loop(0, 4, down_theirs, 0)

    def down_mine(j, _):
        mine = down_part(tp, j).astype(F32)
        to_partner(down_out.at[j], down_in.at[j], 9 + j).wait_recv()
        cols = pl.ds(pl.multiple_of(j * 256, 256), 256)
        summed = mine + down_in[j].astype(F32)
        out[:, cols] = (tok[tp, :, cols].astype(F32) + summed).astype(BF16)
        return 0

    lax.fori_loop(0, 4, down_mine, 0)
    for j in range(8):
        to_partner(mix_out.at[j], mix_in.at[j], 1 + j).wait_send()
    for j in range(4):
        to_partner(down_out.at[j], down_in.at[j], 9 + j).wait_send()
    g.leave()


def local(
    tokens,
    first_norm_gain,
    query_projection_weight,
    key_projection_weight,
    value_projection_weight,
    output_gate_weight,
    decay_projection_weight,
    fading_shift_vector,
    added_fading_exponent,
    per_head_gain,
    mixer_result_matrix,
    second_norm_gain,
    up_linear_weight,
    up_gating_weight,
    depthwise_taps,
    depthwise_bias,
    down_projection_weight,
):
    any_spec = pl.BlockSpec(memory_space=pl.ANY)
    vmem_spec = pl.BlockSpec(memory_space=pltpu.VMEM)
    dma = pltpu.SemaphoreType.DMA
    return pl.pallas_call(
        layer_kernel,
        out_shape=pltpu.VMEM((ROWS, HALF), BF16),
        in_specs=[any_spec] * 11 + [vmem_spec] * 6,
        out_specs=vmem_spec,
        scratch_shapes=[
            pltpu.VMEM((2, 4, 4, 64, COLS), BF16),
            pltpu.VMEM((8, 2048), F32),
            pltpu.VMEM((2, ROWS, HALF), BF16),
            pltpu.VMEM((ROWS, 2048), BF16),
            pltpu.VMEM((ROWS, 1536), BF16),
            pltpu.VMEM((ROWS, 256), F32),
            pltpu.VMEM((ROWS, 256), F32),
            pltpu.VMEM((ROWS, 512), BF16),
            pltpu.VMEM((8, ROWS, 256), BF16),
            pltpu.VMEM((8, ROWS, 256), BF16),
            pltpu.VMEM((ROWS, FF), BF16),
            pltpu.VMEM((4, ROWS, 256), BF16),
            pltpu.VMEM((4, ROWS, 256), BF16),
            dma((NSEM,)),
            dma((NSEM,)),
            dma((11,)),
            dma((13,)),
            dma((13,)),
        ],
        compiler_params=pltpu.CompilerParams(
            collective_id=0, has_side_effects=True, vmem_limit_bytes=LIMIT
        ),
        name="layer",
    )(
        tokens,
        query_projection_weight,
        key_projection_weight,
        value_projection_weight,
        output_gate_weight,
        decay_projection_weight,
        mixer_result_matrix.T,
        up_linear_weight,
        up_gating_weight,
        down_projection_weight.T,
        added_fading_exponent,
        first_norm_gain,
        fading_shift_vector[None],
        per_head_gain,
        second_norm_gain,
        depthwise_taps.transpose(1, 0, 2),
        depthwise_bias,
    )


def solution(mesh):
    return jax.shard_map(
        local,
        mesh=mesh,
        in_specs=(
            P(("rep", "fs"), "tp"),
            P(),
            P("fs", "tp"),
            P("fs", "tp"),
            P("fs", "tp"),
            P("fs", "tp"),
            P("fs", "tp"),
            P("tp"),
            P(("rep", "fs"), "tp"),
            P(),
            P("tp", "fs"),
            P(),
            P("fs", "tp"),
            P("fs", "tp"),
            P(None, None, "tp"),
            P(None, "tp"),
            P("tp", "fs"),
        ),
        out_specs=P(("rep", "fs"), "tp"),
        check_vma=False,
    )
```

```python
import jax
import jax.numpy as jnp
from jax import lax
from jax.experimental import pallas as pl
from jax.experimental.pallas import tpu as pltpu
from jax.sharding import PartitionSpec as P

LANE = 128
MESH = pl.DeviceIdType.MESH
GROUPS = ((0, (6, 7, 3, 2)), (18, (8, 7, 4, 5)), (42, (3, 3, 3, 3)))
COLS = 54 * LANE
CLASSES = (("x", 1, True), ("y", -1, True), ("x", 1, False), ("y", -1, False))
NSEM = 144


class Gather:
    def __init__(self, full, send_sem, recv_sem):
        self.full, self.send_sem, self.recv_sem = full, send_sem, recv_sem
        rep, fs, self.tp = (lax.axis_index(a) for a in ("rep", "fs", "tp"))
        self.x, self.y, self.l = lax.rem(fs, 4), lax.rem(fs // 4, 4), fs // 16
        self.z = rep * 2 + self.l
        self.ids, self.sent = {}, {}

    def device(self, dim, step):
        x, y, z = self.x, self.y, self.z
        if dim == "x":
            x = lax.rem(x + step + 4, 4)
        elif dim == "y":
            y = lax.rem(y + step + 4, 4)
        else:
            z = lax.rem(z + step + 4, 4)
        return (z // 2, lax.rem(z, 2) * 16 + y * 4 + x, self.tp)

    def neighbours(self):
        return [self.device(d, s) for d in "xyz" for s in (1, -1)] + [
            (self.z // 2, self.l * 16 + self.y * 4 + self.x, 1 - self.tp)
        ]

    def cols(self, g, c):
        at, widths = GROUPS[g]
        return pl.ds((at + sum(widths[:c])) * LANE, widths[c] * LANE)

    def piece(self, g, c, stage, off, half=None, z=None):
        first, _, last = CLASSES[c]
        if z is None:
            zs = pl.ds(self.l, 1) if last else pl.ds(0, 2)
        else:
            zs = pl.ds(z, 1)
        rows = pl.ds(0, 64) if half is None else pl.ds(32 * half, 32)
        dim = first if stage == 1 else ("y" if first == "x" else "x")
        mine = self.x if dim == "x" else self.y
        at = pl.ds(lax.rem(mine + off + 4, 4), 1)
        if stage == 1:
            other = pl.ds(self.y if dim == "x" else self.x, 1)
        else:
            other = pl.ds(0, 4)
        yx = (other, at) if dim == "x" else (at, other)
        return self.full.at[zs, yx[0], yx[1], rows, self.cols(g, c)]

    def copy(self, key, ref, dim, step):
        i = self.ids.setdefault(key, len(self.ids))
        return pltpu.make_async_remote_copy(
            src_ref=ref,
            dst_ref=ref,
            send_sem=self.send_sem.at[i],
            recv_sem=self.recv_sem.at[i],
            device_id=self.device(dim, step),
            device_id_type=MESH,
        )

    def send(self, key, ref_args, dim, step):
        copy = self.copy(key, self.piece(*ref_args), dim, step)
        copy.start()
        self.sent[key] = (ref_args, dim, step)

    def recv(self, key, ref):
        self.copy(key, ref, "x", 1).wait_recv()

    def dim(self, c, stage):
        first = CLASSES[c][0]
        return first if stage == 1 else ("y" if first == "x" else "x")

    def hop_one(self, g, c, stage):
        own = (g, c, stage, 0)
        self.send((g, c, stage, "f1"), own, self.dim(c, stage), 1)
        self.send((g, c, stage, "b1"), own, self.dim(c, stage), -1)

    def hop_two(self, g, c, stage):
        d = self.dim(c, stage)
        self.recv((g, c, stage, "f1"), self.piece(g, c, stage, -1))
        self.send((g, c, stage, "f2"), (g, c, stage, -1, 0), d, 1)
        self.recv((g, c, stage, "b1"), self.piece(g, c, stage, 1))
        self.send((g, c, stage, "b2"), (g, c, stage, 1, 1), d, -1)

    def hop_end(self, g, c, stage):
        self.recv((g, c, stage, "f2"), self.piece(g, c, stage, 2, 0))
        self.recv((g, c, stage, "b2"), self.piece(g, c, stage, 2, 1))

    def zkey(self, g, c, stage, off):
        return (g, c, stage, "z", off)

    def zsend(self, g, c, stage, off):
        self.send(
            self.zkey(g, c, stage, off),
            (g, c, stage, off, None, self.l),
            "z",
            CLASSES[c][1],
        )

    def zrecv(self, g, c, stage, off):
        self.recv(
            self.zkey(g, c, stage, off), self.piece(g, c, stage, off, z=1 - self.l)
        )

    def unit(self, g, c, k):
        last = CLASSES[c][2]
        if k == 0:
            if last:
                self.hop_one(g, c, 1)
            self.zsend(g, c, 1, 0)
        elif k == 1:
            self.zrecv(g, c, 1, 0)
            self.hop_one(g, c, 1)
        elif k in (2, 3, 6, 7):
            stage = 1 if k < 4 else 2
            self.hop_two(g, c, stage)
            if last:
                self.zsend(g, c, stage, -1)
                self.zsend(g, c, stage, 1)
        elif k in (4, 5):
            self.hop_end(g, c, 1)
            self.hop_one(g, c, 2)
            if last:
                self.zsend(g, c, 1, 2)
        elif k == 8:
            self.hop_end(g, c, 2)
            self.zsend(g, c, 2, 2)

    def gathered(self, g, classes=(2, 3, 0, 1)):
        for c in classes:
            if not CLASSES[c][2]:
                self.hop_end(g, c, 2)
                continue
            for off in (0, -1, 1, 2):
                self.zrecv(g, c, 1, off)
            for off in (-1, 1, 2):
                self.zrecv(g, c, 2, off)

    def enter(self):
        barrier = pltpu.get_barrier_semaphore()
        for d in self.neighbours():
            pl.semaphore_signal(barrier, inc=1, device_id=d, device_id_type=MESH)
        pl.semaphore_wait(barrier, 7)

    def partner(self):
        return (self.z // 2, self.l * 16 + self.y * 4 + self.x, 1 - self.tp)

    def steps(self, phase, i=0):
        for todo in PLAN.get(phase, {}).get(i, ()):
            self.unit(*todo)

    def steps_in(self, i, phase, every=1, start=0):
        for at in sorted(set(PLAN.get(phase, {})) - set(range(start))):

            @pl.when(i == at * every + every - 1)
            def _():
                self.steps(phase, at)

    def leave(self):
        for key, (ref_args, dim, step) in self.sent.items():
            self.copy(key, self.piece(*ref_args), dim, step).wait_send()


LIMIT = 65011712
ROWS = 768
SEQ = 256
HALF = 1024
NORM_EPS = 1e-06
VALUE_DIM = 128
SHARPNESS = 16.0
MIX_AT, UP_AT, DOWN_AT, FF = 1792, 2304, 5376, 1536
ROW_STEP = 128
PER_UNIT = ROWS // ROW_STEP // 6
F32, BF16 = jnp.float32, jnp.bfloat16

PLAN = {
    'open': {
        0: [(0, 3, 0), (0, 0, 0), (0, 1, 0), (0, 2, 0)],
    },
    'norm': {
        0: [(1, 0, 0), (1, 3, 0), (1, 1, 0), (0, 0, 2), (0, 1, 2), (0, 2, 1)],
        2: [(1, 2, 0), (0, 3, 1), (1, 0, 2), (2, 3, 0), (2, 2, 0), (1, 1, 2), (0, 0, 4), (0, 1, 4), (0, 3, 3)],
        3: [(1, 3, 1), (0, 2, 3)],
        4: [(0, 0, 6), (1, 1, 4), (0, 3, 5), (0, 2, 5), (0, 1, 6), (2, 1, 0), (2, 2, 1), (2, 0, 0), (1, 2, 1), (0, 0, 8), (1, 0, 4), (0, 3, 7), (1, 3, 3)],
        5: [(0, 1, 8), (0, 2, 7), (1, 1, 6), (1, 0, 6), (1, 2, 3), (1, 3, 5), (2, 3, 1), (1, 1, 8)],
    },
    'project': {
        0: [(2, 1, 2), (1, 2, 5), (1, 0, 8)],
        2: [(2, 0, 2), (2, 2, 3)],
        3: [(2, 3, 3)],
    },
    'heads': {
        0: [(2, 1, 4)],
        4: [(2, 0, 4)],
    },
    'mix': {
        0: [(1, 3, 7)],
        4: [(2, 3, 5)],
        6: [(1, 2, 7), (2, 2, 5)],
    },
    'mixed': {
        0: [(2, 1, 6)],
    },
    'got1': {
        0: [(2, 0, 6)],
    },
    'up': {
        2: [(2, 3, 7), (2, 2, 7)],
        3: [(2, 1, 8), (2, 0, 8)],
    },
}


def dot(a, b):
    return jnp.dot(a, b, preferred_element_type=F32)


def dot_nt(a, b):
    return lax.dot_general(a, b, (((1,), (1,)), ((), ())), preferred_element_type=F32)


def normalize(parts, gain_ref):
    total = sum(jnp.sum(p * p, axis=-1, keepdims=True) for p in parts)
    scale = lax.rsqrt(total * (1.0 / 2048) + NORM_EPS)
    width = 2048 // len(parts)
    return [
        (p * scale * gain_ref[:, i * width : (i + 1) * width]).astype(BF16)
        for i, p in enumerate(parts)
    ]


def head_pair(s, pair, qkvg, decay, mixed, head_gain):
    rows = pl.ds(pl.multiple_of(s * SEQ, SEQ), SEQ)
    at = pl.multiple_of(pair * LANE, LANE)
    lane = lax.broadcasted_iota(jnp.int32, (1, LANE), 1)
    low = lane < 64
    t = lax.broadcasted_iota(jnp.int32, (SEQ, SEQ), 0)
    u = lax.broadcasted_iota(jnp.int32, (SEQ, SEQ), 1)
    before = u <= t
    after = u >= t

    log_a = decay[rows, pl.ds(at, LANE)]
    ones = before.astype(F32).astype(BF16)
    high = log_a.astype(BF16)
    rest = log_a - high.astype(F32)
    middle = rest.astype(BF16)
    small = (rest - middle.astype(F32)).astype(BF16)
    done = dot(ones, high) + (dot(ones, middle) + dot(ones, small))
    open_ = done - log_a
    mid = [done[64 * b + 31 : 64 * b + 32] for b in range(4)]
    mid_open = [open_[64 * b + 32 : 64 * b + 33] for b in range(4)]

    q = qkvg[rows, pl.ds(at, LANE)].astype(F32) * 0.125
    k = qkvg[rows, pl.ds(pl.multiple_of(at + 256, LANE), LANE)].astype(F32)
    blocks = [slice(64 * b, 64 * b + 64) for b in range(4)]
    key_fwd = [k[r] * jnp.exp(mid[b] - done[r]) for b, r in enumerate(blocks)]
    key_bwd = [k[r] * jnp.exp(open_[r] - mid_open[b]) for b, r in enumerate(blocks)]

    def swap(v):
        return pltpu.roll(v, 64, 1)

    def both(v, parity):
        other = swap(v)
        return jnp.where(low, v, other) if parity == 0 else jnp.where(low, other, v)

    nothing = jnp.zeros((64, LANE), BF16)

    def side(queries, points, mids, keys, backward, parity):
        sign = -1.0 if backward else 1.0
        point_mids = [
            jnp.where(low, both(mids[2 * p], parity), both(mids[2 * p + 1], parity))
            for p in range(2)
        ]
        left, right = [], []
        for b, r in enumerate(blocks):
            row = []
            for p in range(2):
                expo = (points[r] - point_mids[p]) * sign
                if backward:
                    used = (b <= 2 * p, b <= 2 * p + 1)
                else:
                    used = (b >= 2 * p, b >= 2 * p + 1)
                if not any(used):
                    row.append(nothing)
                    continue
                if not all(used):
                    expo = jnp.where(low if used[0] else ~low, expo, -1e30)
                row.append((queries[r] * jnp.exp(expo)).astype(BF16))
            left.append(jnp.concatenate(row, axis=1))
            mine = keys[b] if parity == b % 2 else swap(keys[b])
            mine = jnp.where(low if b % 2 == 0 else ~low, mine, 0.0).astype(BF16)
            right.append(
                jnp.concatenate([mine if p == b // 2 else nothing for p in range(2)], axis=1)
            )
        return dot_nt(jnp.concatenate(left, axis=0), jnp.concatenate(right, axis=0))

    for parity in range(2):
        queries = both(q, parity)
        fwd = side(queries, both(done, parity), mid, key_fwd, False, parity)
        bwd = side(queries, both(open_, parity), mid_open, key_bwd, True, parity)
        scores = jnp.where(before, fwd, 0.0) + jnp.where(after, bwd, 0.0)
        place = pl.multiple_of(pair * 256 + parity * LANE, LANE)
        values = qkvg[rows, pl.ds(pl.multiple_of(place + 512, LANE), LANE)]
        out = dot(scores.astype(BF16), values)
        scale = lax.rsqrt(jnp.mean(out * out, axis=-1, keepdims=True) + NORM_EPS)
        out = out * scale * head_gain[...]
        gate = qkvg[rows, pl.ds(pl.multiple_of(place + 1024, LANE), LANE)].astype(F32)
        out = out * (gate * jax.nn.sigmoid(gate))
        mixed[rows, pl.ds(place, LANE)] = out.astype(BF16)


def smooth(source, taps, bias):
    row = lax.broadcasted_iota(jnp.int32, source.shape, 0)
    back = jnp.where(row == 0, 0.0, pltpu.roll(source, 1, 0))
    ahead = jnp.where(row == SEQ - 1, 0.0, pltpu.roll(source, SEQ - 1, 0))
    return bias + back * taps[0:1] + source * taps[1:2] + ahead * taps[2:3]


def layer_kernel(
    tokens,
    wq,
    wk,
    wv,
    wg,
    wd,
    mix_t,
    up_lin,
    up_gate,
    down_t,
    added,
    gain_one,
    shift,
    head_gain,
    gain_two,
    taps,
    bias,
    out,
    full,
    gains,
    tok,
    normed,
    qkvg,
    decay,
    fading,
    mixed,
    mix_out,
    mix_in,
    hidden,
    down_out,
    down_in,
    partial,
    send_sem,
    recv_sem,
    load_sem,
    pair_send,
    pair_recv,
):
    g = Gather(full, send_sem, recv_sem)
    tp = g.tp
    own = full.at[g.l, g.y, g.x]
    loads = [pltpu.make_async_copy(tokens, tok.at[tp], load_sem.at[0])]
    at = 0
    for n, w in enumerate((wq, wk, wv, wg, wd, mix_t, up_lin, up_gate, down_t)):
        width = w.shape[1]
        loads.append(
            pltpu.make_async_copy(w, own.at[:, pl.ds(at, width)], load_sem.at[n + 1])
        )
        at += width
    fading_load = pltpu.make_async_copy(added, fading, load_sem.at[10])
    for load in loads:
        load.start()
    fading_load.start()
    gains[0:1] = gain_one[...].astype(F32)[None]
    gains[1:2] = gain_two[...].astype(F32)[None]
    gains[2:3, :VALUE_DIM] = head_gain[...].astype(F32)[None]
    gain_one, gain_two = gains.at[0:1], gains.at[1:2]
    head_gain = gains.at[2:3, :VALUE_DIM]
    g.enter()

    def to_partner(src, dst, n):
        return pltpu.make_async_remote_copy(
            src_ref=src,
            dst_ref=dst,
            send_sem=pair_send.at[n],
            recv_sem=pair_recv.at[n],
            device_id=g.partner(),
            device_id_type=MESH,
        )

    for load in loads[1:]:
        load.wait()
    g.steps("open")
    loads[0].wait()
    swap_tokens = to_partner(tok.at[tp], tok.at[tp], 0)
    swap_tokens.start()
    fading_load.wait()
    to_partner(tok.at[tp], tok.at[1 - tp], 0).wait_recv()

    def first_norm(i, _):
        rows = pl.ds(pl.multiple_of(i * ROW_STEP, ROW_STEP), ROW_STEP)
        parts = normalize([tok[h, rows, :].astype(F32) for h in range(2)], gain_one)
        for h in range(2):
            normed[rows, h * HALF : (h + 1) * HALF] = parts[h]
        g.steps_in(i, "norm", PER_UNIT)
        return 0

    lax.fori_loop(0, ROWS // ROW_STEP, first_norm, 0)
    g.gathered(0)
    g.steps("got0")

    score = dot(normed[...], full[:, :, :, :, 1536:1792].reshape(2048, 256)) + shift[...]
    faded = jnp.minimum(score, 0.0) - jnp.log1p(jnp.exp(-jnp.abs(score)))
    decay[...] = faded * (1.0 / SHARPNESS) + fading[...]

    g.steps("project")

    def project(j, _):
        cols = pl.ds(pl.multiple_of(j * 256, 256), 256)
        weight = full[:, :, :, :, cols].reshape(2048, 256)
        qkvg[:, cols] = dot(normed[...], weight).astype(BF16)
        g.steps_in(j + 1, "project", 1, 1)
        return 0

    lax.fori_loop(0, 6, project, 0)

    def heads(i, _):
        head_pair(i // 2, lax.rem(i, 2), qkvg, decay, mixed, head_gain)
        g.steps_in(i, "heads")
        return 0

    lax.fori_loop(0, 6, heads, 0)

    def mix(j, _):
        weight = full[j // 4, lax.rem(j, 4), :, :, MIX_AT:UP_AT].reshape(256, 512)
        mix_out[j] = dot_nt(mixed[...], weight).astype(BF16)
        to_partner(mix_out.at[j], mix_in.at[j], 1 + j).start()
        g.steps_in(j, "mix")
        return 0

    lax.fori_loop(0, 8, mix, 0)
    for j in range(8):
        to_partner(mix_out.at[j], mix_in.at[j], 1 + j).wait_recv()
    g.steps("mixed")

    def second_norm(i, _):
        rows = pl.ds(pl.multiple_of(i * ROW_STEP, ROW_STEP), ROW_STEP)
        parts = []
        for j in range(8):
            cols = slice((j % 4) * 256, (j % 4 + 1) * 256)
            term = mix_out[j, rows, :].astype(F32) + mix_in[j, rows, :].astype(F32)
            kept = (tok[j // 4, rows, cols].astype(F32) + term).astype(BF16)
            tok[j // 4, rows, cols] = kept
            parts.append(kept.astype(F32))
        for j, part in enumerate(normalize(parts, gain_two)):
            normed[rows, j * 256 : (j + 1) * 256] = part
        g.steps_in(i, "second", PER_UNIT)
        return 0

    swap_tokens.wait_send()
    lax.fori_loop(0, ROWS // ROW_STEP, second_norm, 0)
    g.gathered(1)
    g.steps("got1")

    def up(j, _):
        cols = pl.ds(pl.multiple_of(j * 256, 256), 256)
        parts = []
        for half in range(2):
            at = pl.multiple_of(UP_AT + half * FF + j * 256, 256)
            weight = full[:, :, :, :, pl.ds(at, 256)].reshape(2048, 256)
            parts.append(dot(normed[...], weight).astype(BF16))
        tap = [taps[:, half, cols].astype(F32) for half in range(2)]
        base = bias[:, cols].astype(F32)
        for s in range(ROWS // SEQ):
            rows = slice(s * SEQ, (s + 1) * SEQ)
            lin, gate = (
                smooth(parts[h][rows].astype(F32), tap[h], base[h : h + 1]) for h in range(2)
            )
            hidden[rows, cols] = (lin * (gate * jax.nn.sigmoid(gate))).astype(BF16)
        g.steps_in(j, "up")
        return 0

    lax.fori_loop(0, FF // 256, up, 0)
    late = sum(GROUPS[2][1][:2]) * LANE

    def down_part(half, j, low, high):
        pair = pl.ds(pl.multiple_of(2 * j, 2), 2)
        weight = full[half, pair, :, :, DOWN_AT + low : DOWN_AT + high]
        return dot_nt(hidden[:, low:high], weight.reshape(512, high - low))

    def down_early(i, _):
        half = lax.rem(1 - tp + i // 2, 2)
        partial[i] = down_part(half, lax.rem(i, 2), late, FF)
        g.steps_in(i, "downa")
        return 0

    g.gathered(2, (2, 3))
    g.steps("got2a")
    lax.fori_loop(0, 4, down_early, 0)
    g.gathered(2, (0, 1))

    def down_theirs(j, _):
        down_out[j] = (partial[j] + down_part(1 - tp, j, 0, late)).astype(BF16)
        to_partner(down_out.at[j], down_in.at[j], 9 + j).start()
        return 0

    lax.fori_loop(0, 2, down_theirs, 0)

    def down_mine(j, _):
        mine = (partial[j + 2] + down_part(tp, j, 0, late)).astype(BF16).astype(F32)
        to_partner(down_out.at[j], down_in.at[j], 9 + j).wait_recv()
        cols = pl.ds(pl.multiple_of(j * 512, 512), 512)
        summed = mine + down_in[j].astype(F32)
        out[:, cols] = (tok[tp, :, cols].astype(F32) + summed).astype(BF16)
        return 0

    lax.fori_loop(0, 2, down_mine, 0)
    for j in range(8):
        to_partner(mix_out.at[j], mix_in.at[j], 1 + j).wait_send()
    for j in range(2):
        to_partner(down_out.at[j], down_in.at[j], 9 + j).wait_send()
    g.leave()


def local(
    tokens,
    first_norm_gain,
    query_projection_weight,
    key_projection_weight,
    value_projection_weight,
    output_gate_weight,
    decay_projection_weight,
    fading_shift_vector,
    added_fading_exponent,
    per_head_gain,
    mixer_result_matrix,
    second_norm_gain,
    up_linear_weight,
    up_gating_weight,
    depthwise_taps,
    depthwise_bias,
    down_projection_weight,
):
    any_spec = pl.BlockSpec(memory_space=pl.ANY)
    vmem_spec = pl.BlockSpec(memory_space=pltpu.VMEM)
    dma = pltpu.SemaphoreType.DMA
    return pl.pallas_call(
        layer_kernel,
        out_shape=pltpu.VMEM((ROWS, HALF), BF16),
        in_specs=[any_spec] * 11 + [vmem_spec] * 6,
        out_specs=vmem_spec,
        scratch_shapes=[
            pltpu.VMEM((2, 4, 4, 64, COLS), BF16),
            pltpu.VMEM((8, 2048), F32),
            pltpu.VMEM((2, ROWS, HALF), BF16),
            pltpu.VMEM((ROWS, 2048), BF16),
            pltpu.VMEM((ROWS, 1536), BF16),
            pltpu.VMEM((ROWS, 256), F32),
            pltpu.VMEM((ROWS, 256), F32),
            pltpu.VMEM((ROWS, 512), BF16),
            pltpu.VMEM((8, ROWS, 256), BF16),
            pltpu.VMEM((8, ROWS, 256), BF16),
            pltpu.VMEM((ROWS, FF), BF16),
            pltpu.VMEM((2, ROWS, 512), BF16),
            pltpu.VMEM((2, ROWS, 512), BF16),
            pltpu.VMEM((4, ROWS, 512), F32),
            dma((NSEM,)),
            dma((NSEM,)),
            dma((11,)),
            dma((11,)),
            dma((11,)),
        ],
        compiler_params=pltpu.CompilerParams(
            collective_id=0, has_side_effects=True, vmem_limit_bytes=LIMIT
        ),
        name="layer",
    )(
        tokens,
        query_projection_weight,
        key_projection_weight,
        value_projection_weight,
        output_gate_weight,
        decay_projection_weight,
        mixer_result_matrix.T,
        up_linear_weight,
        up_gating_weight,
        down_projection_weight.T,
        added_fading_exponent,
        first_norm_gain,
        fading_shift_vector[None],
        per_head_gain,
        second_norm_gain,
        depthwise_taps.transpose(1, 0, 2),
        depthwise_bias,
    )


def solution(mesh):
    return jax.shard_map(
        local,
        mesh=mesh,
        in_specs=(
            P(("rep", "fs"), "tp"),
            P(),
            P("fs", "tp"),
            P("fs", "tp"),
            P("fs", "tp"),
            P("fs", "tp"),
            P("fs", "tp"),
            P("tp"),
            P(("rep", "fs"), "tp"),
            P(),
            P("tp", "fs"),
            P(),
            P("fs", "tp"),
            P("fs", "tp"),
            P(None, None, "tp"),
            P(None, "tp"),
            P("tp", "fs"),
        ),
        out_specs=P(("rep", "fs"), "tp"),
        check_vma=False,
    )
```

```python
import jax
import jax.numpy as jnp
from jax import lax
from jax.experimental import pallas as pl
from jax.experimental.pallas import tpu as pltpu
from jax.sharding import PartitionSpec as P

LANE = 128
MESH = pl.DeviceIdType.MESH
GROUPS = ((0, (6, 6, 3, 3)), (18, (8, 8, 4, 4)), (42, (3, 3, 3, 3)))
COLS = 54 * LANE
CLASSES = (("x", 1, True), ("y", -1, True), ("x", 1, False), ("y", -1, False))
NSEM = 144


class Gather:
    def __init__(self, full, send_sem, recv_sem):
        self.full, self.send_sem, self.recv_sem = full, send_sem, recv_sem
        rep, fs, self.tp = (lax.axis_index(a) for a in ("rep", "fs", "tp"))
        self.x, self.y, self.l = lax.rem(fs, 4), lax.rem(fs // 4, 4), fs // 16
        self.z = rep * 2 + self.l
        self.ids, self.sent = {}, {}

    def device(self, dim, step):
        x, y, z = self.x, self.y, self.z
        if dim == "x":
            x = lax.rem(x + step + 4, 4)
        elif dim == "y":
            y = lax.rem(y + step + 4, 4)
        else:
            z = lax.rem(z + step + 4, 4)
        return (z // 2, lax.rem(z, 2) * 16 + y * 4 + x, self.tp)

    def neighbours(self):
        return [self.device(d, s) for d in "xyz" for s in (1, -1)] + [
            (self.z // 2, self.l * 16 + self.y * 4 + self.x, 1 - self.tp)
        ]

    def cols(self, g, c):
        at, widths = GROUPS[g]
        return pl.ds((at + sum(widths[:c])) * LANE, widths[c] * LANE)

    def piece(self, g, c, stage, off, half=None, z=None):
        first, _, last = CLASSES[c]
        if z is None:
            zs = pl.ds(self.l, 1) if last else pl.ds(0, 2)
        else:
            zs = pl.ds(z, 1)
        rows = pl.ds(0, 64) if half is None else pl.ds(32 * half, 32)
        dim = first if stage == 1 else ("y" if first == "x" else "x")
        mine = self.x if dim == "x" else self.y
        at = pl.ds(lax.rem(mine + off + 4, 4), 1)
        if stage == 1:
            other = pl.ds(self.y if dim == "x" else self.x, 1)
        else:
            other = pl.ds(0, 4)
        yx = (other, at) if dim == "x" else (at, other)
        return self.full.at[zs, yx[0], yx[1], rows, self.cols(g, c)]

    def copy(self, key, ref, dim, step):
        i = self.ids.setdefault(key, len(self.ids))
        return pltpu.make_async_remote_copy(
            src_ref=ref,
            dst_ref=ref,
            send_sem=self.send_sem.at[i],
            recv_sem=self.recv_sem.at[i],
            device_id=self.device(dim, step),
            device_id_type=MESH,
        )

    def send(self, key, ref_args, dim, step):
        copy = self.copy(key, self.piece(*ref_args), dim, step)
        copy.start()
        self.sent[key] = (ref_args, dim, step)

    def recv(self, key, ref):
        self.copy(key, ref, "x", 1).wait_recv()

    def dim(self, c, stage):
        first = CLASSES[c][0]
        return first if stage == 1 else ("y" if first == "x" else "x")

    def hop_one(self, g, c, stage):
        own = (g, c, stage, 0)
        self.send((g, c, stage, "f1"), own, self.dim(c, stage), 1)
        self.send((g, c, stage, "b1"), own, self.dim(c, stage), -1)

    def hop_two(self, g, c, stage):
        d = self.dim(c, stage)
        self.recv((g, c, stage, "f1"), self.piece(g, c, stage, -1))
        self.send((g, c, stage, "f2"), (g, c, stage, -1, 0), d, 1)
        self.recv((g, c, stage, "b1"), self.piece(g, c, stage, 1))
        self.send((g, c, stage, "b2"), (g, c, stage, 1, 1), d, -1)

    def hop_end(self, g, c, stage):
        self.recv((g, c, stage, "f2"), self.piece(g, c, stage, 2, 0))
        self.recv((g, c, stage, "b2"), self.piece(g, c, stage, 2, 1))

    def zkey(self, g, c, stage, off):
        return (g, c, stage, "z", off)

    def zsend(self, g, c, stage, off):
        self.send(
            self.zkey(g, c, stage, off),
            (g, c, stage, off, None, self.l),
            "z",
            CLASSES[c][1],
        )

    def zrecv(self, g, c, stage, off):
        self.recv(
            self.zkey(g, c, stage, off), self.piece(g, c, stage, off, z=1 - self.l)
        )

    def unit(self, g, c, k):
        last = CLASSES[c][2]
        if k == 0:
            if last:
                self.hop_one(g, c, 1)
            self.zsend(g, c, 1, 0)
        elif k == 1:
            self.zrecv(g, c, 1, 0)
            self.hop_one(g, c, 1)
        elif k in (2, 3, 6, 7):
            stage = 1 if k < 4 else 2
            self.hop_two(g, c, stage)
            if last:
                self.zsend(g, c, stage, -1)
                self.zsend(g, c, stage, 1)
        elif k in (4, 5):
            self.hop_end(g, c, 1)
            self.hop_one(g, c, 2)
            if last:
                self.zsend(g, c, 1, 2)
        elif k == 8:
            self.hop_end(g, c, 2)
            self.zsend(g, c, 2, 2)

    def gathered(self, g, classes=(2, 3, 0, 1)):
        for c in classes:
            if not CLASSES[c][2]:
                self.hop_end(g, c, 2)
                continue
            for off in (0, -1, 1, 2):
                self.zrecv(g, c, 1, off)
            for off in (-1, 1, 2):
                self.zrecv(g, c, 2, off)

    def enter(self):
        barrier = pltpu.get_barrier_semaphore()
        for d in self.neighbours():
            pl.semaphore_signal(barrier, inc=1, device_id=d, device_id_type=MESH)
        pl.semaphore_wait(barrier, 7)

    def partner(self):
        return (self.z // 2, self.l * 16 + self.y * 4 + self.x, 1 - self.tp)

    def steps(self, phase, i=0):
        for todo in PLAN.get(phase, {}).get(i, ()):
            self.unit(*todo)

    def steps_in(self, i, phase, every=1, start=0, stop=99):
        for at in sorted(set(PLAN.get(phase, {})) & set(range(start, stop))):

            @pl.when(i == at * every + every - 1)
            def _():
                self.steps(phase, at)

    def leave(self):
        for key, (ref_args, dim, step) in self.sent.items():
            self.copy(key, self.piece(*ref_args), dim, step).wait_send()


LIMIT = 65011712
ROWS = 768
SEQ = 256
HALF = 1024
NORM_EPS = 1e-06
VALUE_DIM = 128
SHARPNESS = 16.0
MIX_AT, UP_AT, DOWN_AT, FF = 1792, 2304, 5376, 1536
ROW_STEP = 128
PER_UNIT = ROWS // ROW_STEP // 6
F32, BF16 = jnp.float32, jnp.bfloat16

PLAN = {
    'open': {
        0: [(2, 3, 0), (0, 2, 0), (0, 0, 0), (0, 3, 0), (0, 1, 0), (1, 2, 0), (2, 1, 0), (1, 0, 0), (1, 1, 0), (0, 0, 2), (0, 2, 1), (1, 3, 0), (0, 1, 2)],
    },
    'norm': {
        0: [(0, 3, 1), (2, 2, 0), (2, 0, 0)],
        1: [(2, 1, 2), (1, 2, 1), (0, 0, 4), (1, 1, 2), (0, 2, 3), (0, 3, 3)],
        2: [(0, 1, 4), (0, 2, 5), (1, 0, 2)],
        3: [(1, 3, 1), (2, 0, 2), (0, 3, 5), (0, 1, 6), (0, 0, 6), (1, 0, 4)],
        4: [(1, 1, 4)],
        5: [(0, 0, 8), (1, 3, 3), (1, 2, 3), (0, 1, 8), (0, 3, 7), (2, 2, 1), (0, 2, 7), (1, 3, 5), (1, 1, 6), (1, 2, 5), (1, 0, 6)],
    },
    'project': {
        6: [(2, 3, 1)],
    },
    'heads': {
        1: [(1, 2, 7), (2, 2, 3)],
        4: [(1, 3, 7)],
    },
    'mix': {
        2: [(2, 1, 4), (1, 0, 8)],
        4: [(2, 3, 3), (1, 1, 8), (2, 0, 4)],
    },
    'second': {
        0: [(2, 2, 5)],
        1: [(2, 3, 5)],
    },
    'up': {
        0: [(2, 0, 6)],
        4: [(2, 1, 8), (2, 0, 8)],
    },
    'got1b': {
        0: [(2, 1, 6)],
    },
    'got1c': {
        0: [(2, 3, 7), (2, 2, 7)],
    },
}


def dot(a, b):
    return jnp.dot(a, b, preferred_element_type=F32)


def dot_nt(a, b):
    return lax.dot_general(a, b, (((1,), (1,)), ((), ())), preferred_element_type=F32)


def normalize(parts, gain_ref):
    total = sum(jnp.sum(p * p, axis=-1, keepdims=True) for p in parts)
    scale = lax.rsqrt(total * (1.0 / 2048) + NORM_EPS)
    width = 2048 // len(parts)
    return [
        (p * scale * gain_ref[:, i * width : (i + 1) * width]).astype(BF16)
        for i, p in enumerate(parts)
    ]


def head_pair(s, pair, qkvg, decay, mixed, head_gain):
    rows = pl.ds(pl.multiple_of(s * SEQ, SEQ), SEQ)
    at = pl.multiple_of(pair * LANE, LANE)
    lane = lax.broadcasted_iota(jnp.int32, (1, LANE), 1)
    low = lane < 64
    t = lax.broadcasted_iota(jnp.int32, (SEQ, SEQ), 0)
    u = lax.broadcasted_iota(jnp.int32, (SEQ, SEQ), 1)
    before = u <= t
    after = u >= t

    log_a = decay[rows, pl.ds(at, LANE)]
    ones = before.astype(F32).astype(BF16)
    high = log_a.astype(BF16)
    rest = log_a - high.astype(F32)
    middle = rest.astype(BF16)
    small = (rest - middle.astype(F32)).astype(BF16)
    done = dot(ones, high) + (dot(ones, middle) + dot(ones, small))
    open_ = done - log_a
    mid = [done[64 * b + 31 : 64 * b + 32] for b in range(4)]
    mid_open = [open_[64 * b + 32 : 64 * b + 33] for b in range(4)]

    q = qkvg[rows, pl.ds(at, LANE)].astype(F32) * 0.125
    k = qkvg[rows, pl.ds(pl.multiple_of(at + 256, LANE), LANE)].astype(F32)
    blocks = [slice(64 * b, 64 * b + 64) for b in range(4)]
    key_fwd = [k[r] * jnp.exp(mid[b] - done[r]) for b, r in enumerate(blocks)]
    key_bwd = [k[r] * jnp.exp(open_[r] - mid_open[b]) for b, r in enumerate(blocks)]

    def swap(v):
        return pltpu.roll(v, 64, 1)

    def both(v, parity):
        other = swap(v)
        return jnp.where(low, v, other) if parity == 0 else jnp.where(low, other, v)

    nothing = jnp.zeros((64, LANE), BF16)

    def side(queries, points, mids, keys, backward, parity):
        sign = -1.0 if backward else 1.0
        point_mids = [
            jnp.where(low, both(mids[2 * p], parity), both(mids[2 * p + 1], parity))
            for p in range(2)
        ]
        left, right = [], []
        for b, r in enumerate(blocks):
            row = []
            for p in range(2):
                expo = (points[r] - point_mids[p]) * sign
                if backward:
                    used = (b <= 2 * p, b <= 2 * p + 1)
                else:
                    used = (b >= 2 * p, b >= 2 * p + 1)
                if not any(used):
                    row.append(nothing)
                    continue
                if not all(used):
                    expo = jnp.where(low if used[0] else ~low, expo, -1e30)
                row.append((queries[r] * jnp.exp(expo)).astype(BF16))
            left.append(jnp.concatenate(row, axis=1))
            mine = keys[b] if parity == b % 2 else swap(keys[b])
            mine = jnp.where(low if b % 2 == 0 else ~low, mine, 0.0).astype(BF16)
            right.append(
                jnp.concatenate([mine if p == b // 2 else nothing for p in range(2)], axis=1)
            )
        return dot_nt(jnp.concatenate(left, axis=0), jnp.concatenate(right, axis=0))

    for parity in range(2):
        queries = both(q, parity)
        fwd = side(queries, both(done, parity), mid, key_fwd, False, parity)
        bwd = side(queries, both(open_, parity), mid_open, key_bwd, True, parity)
        scores = jnp.where(before, fwd, 0.0) + jnp.where(after, bwd, 0.0)
        place = pl.multiple_of(pair * 256 + parity * LANE, LANE)
        values = qkvg[rows, pl.ds(pl.multiple_of(place + 512, LANE), LANE)]
        out = dot(scores.astype(BF16), values)
        scale = lax.rsqrt(jnp.mean(out * out, axis=-1, keepdims=True) + NORM_EPS)
        out = out * scale * head_gain[...]
        gate = qkvg[rows, pl.ds(pl.multiple_of(place + 1024, LANE), LANE)].astype(F32)
        out = out * (gate * jax.nn.sigmoid(gate))
        mixed[rows, pl.ds(place, LANE)] = out.astype(BF16)


def smooth(source, taps, bias):
    row = lax.broadcasted_iota(jnp.int32, source.shape, 0)
    back = jnp.where(row == 0, 0.0, pltpu.roll(source, 1, 0))
    ahead = jnp.where(row == SEQ - 1, 0.0, pltpu.roll(source, SEQ - 1, 0))
    return bias + back * taps[0:1] + source * taps[1:2] + ahead * taps[2:3]


def layer_kernel(
    tokens,
    wq,
    wk,
    wv,
    wg,
    wd,
    mix_t,
    up_lin,
    up_gate,
    down_t,
    added,
    gain_one,
    shift,
    head_gain,
    gain_two,
    taps,
    bias,
    out,
    full,
    gains,
    tok,
    normed,
    qkvg,
    decay,
    fading,
    mixed,
    mix_out,
    mix_in,
    hidden,
    down_out,
    down_in,
    partial,
    send_sem,
    recv_sem,
    load_sem,
    pair_send,
    pair_recv,
):
    g = Gather(full, send_sem, recv_sem)
    tp = g.tp
    own = full.at[g.l, g.y, g.x]
    loads = [pltpu.make_async_copy(tokens, tok.at[tp], load_sem.at[0])]
    parts = [(w, 0, w.shape[1]) for w in (wq, wk, wv, wg, wd, mix_t)]
    parts += [(w, at, 256) for at in range(0, FF, 256) for w in (up_lin, up_gate)]
    parts += [(down_t, 0, FF)]
    at = 0
    for n, (w, first, width) in enumerate(parts):
        loads.append(
            pltpu.make_async_copy(
                w.at[:, pl.ds(first, width)], own.at[:, pl.ds(at, width)], load_sem.at[n + 1]
            )
        )
        at += width
    fading_load = pltpu.make_async_copy(added, fading, load_sem.at[20])
    for load in loads:
        load.start()
    fading_load.start()
    gains[0:1] = gain_one[...].astype(F32)[None]
    gains[1:2] = gain_two[...].astype(F32)[None]
    gains[2:3, :VALUE_DIM] = head_gain[...].astype(F32)[None]
    gain_one, gain_two = gains.at[0:1], gains.at[1:2]
    head_gain = gains.at[2:3, :VALUE_DIM]
    g.enter()

    def to_partner(src, dst, n):
        return pltpu.make_async_remote_copy(
            src_ref=src,
            dst_ref=dst,
            send_sem=pair_send.at[n],
            recv_sem=pair_recv.at[n],
            device_id=g.partner(),
            device_id_type=MESH,
        )

    for load in loads[1:]:
        load.wait()
    opening = PLAN["open"][0]
    sends = next((n for n, todo in enumerate(opening) if todo[2]), len(opening))
    for todo in opening[:sends]:
        g.unit(*todo)
    loads[0].wait()
    swap_tokens = to_partner(tok.at[tp], tok.at[tp], 0)
    swap_tokens.start()
    for todo in opening[sends:]:
        g.unit(*todo)
    fading_load.wait()
    to_partner(tok.at[tp], tok.at[1 - tp], 0).wait_recv()

    def first_norm(i, _):
        rows = pl.ds(pl.multiple_of(i * ROW_STEP, ROW_STEP), ROW_STEP)
        parts = normalize([tok[h, rows, :].astype(F32) for h in range(2)], gain_one)
        for h in range(2):
            normed[rows, h * HALF : (h + 1) * HALF] = parts[h]
        g.steps_in(i, "norm", PER_UNIT)
        return 0

    lax.fori_loop(0, ROWS // ROW_STEP, first_norm, 0)
    g.gathered(0)
    g.steps("got0")

    score = dot(normed[...], full[:, :, :, :, 1536:1792].reshape(2048, 256)) + shift[...]
    faded = jnp.minimum(score, 0.0) - jnp.log1p(jnp.exp(-jnp.abs(score)))
    decay[...] = faded * (1.0 / SHARPNESS) + fading[...]

    g.steps("project")

    def project(j, _):
        cols = pl.ds(pl.multiple_of(j * 256, 256), 256)
        weight = full[:, :, :, :, cols].reshape(2048, 256)
        qkvg[:, cols] = dot(normed[...], weight).astype(BF16)
        g.steps_in(j + 1, "project", 1, 1)
        return 0

    lax.fori_loop(0, 6, project, 0)

    def heads(i, _):
        head_pair(i // 2, lax.rem(i, 2), qkvg, decay, mixed, head_gain)
        g.steps_in(i, "heads")
        return 0

    lax.fori_loop(0, 6, heads, 0)

    def mix(j, _):
        weight = full[j // 4, lax.rem(j, 4), :, :, MIX_AT:UP_AT].reshape(256, 512)
        mix_out[j] = dot_nt(mixed[...], weight).astype(BF16)
        to_partner(mix_out.at[j], mix_in.at[j], 1 + j).start()
        g.steps_in(j, "mix")
        return 0

    lax.fori_loop(0, 8, mix, 0)
    for j in range(8):
        to_partner(mix_out.at[j], mix_in.at[j], 1 + j).wait_recv()
    g.steps("mixed")

    def second_norm(i, _):
        rows = pl.ds(pl.multiple_of(i * ROW_STEP, ROW_STEP), ROW_STEP)
        parts = []
        for j in range(8):
            cols = slice((j % 4) * 256, (j % 4 + 1) * 256)
            term = mix_out[j, rows, :].astype(F32) + mix_in[j, rows, :].astype(F32)
            kept = (tok[j // 4, rows, cols].astype(F32) + term).astype(BF16)
            tok[j // 4, rows, cols] = kept
            parts.append(kept.astype(F32))
        for j, part in enumerate(normalize(parts, gain_two)):
            normed[rows, j * 256 : (j + 1) * 256] = part
        g.steps_in(i, "second", PER_UNIT)
        return 0

    swap_tokens.wait_send()
    lax.fori_loop(0, ROWS // ROW_STEP, second_norm, 0)
    def up(j, _):
        cols = pl.ds(pl.multiple_of(j * 256, 256), 256)
        at = pl.multiple_of(UP_AT + j * 512, 256)
        weight = full[:, :, :, :, pl.ds(at, 512)].reshape(2048, 512)
        both = dot(normed[...], weight).astype(BF16)
        parts = [both[:, :256], both[:, 256:]]
        tap = [taps[:, half, cols].astype(F32) for half in range(2)]
        base = bias[:, cols].astype(F32)
        for s in range(ROWS // SEQ):
            rows = slice(s * SEQ, (s + 1) * SEQ)
            lin, gate = (
                smooth(parts[h][rows].astype(F32), tap[h], base[h : h + 1]) for h in range(2)
            )
            hidden[rows, cols] = (lin * (gate * jax.nn.sigmoid(gate))).astype(BF16)
        return 0

    done = 0
    for phase, classes, chunks in (
        ("got1a", (2, 3), (4, 6)),
        ("got1b", (0,), (0, 2)),
        ("got1c", (1,), (2, 4)),
    ):
        g.gathered(1, classes)
        g.steps(phase)

        def piece(j, _, shift=done - chunks[0], at=done):
            up(j, 0)
            g.steps_in(j + shift, "up", 1, at, at + 2)
            return 0

        lax.fori_loop(*chunks, piece, 0)
        done += 2

    late = sum(GROUPS[2][1][:2]) * LANE

    def down_part(half, j, low, high):
        pair = pl.ds(pl.multiple_of(2 * j, 2), 2)
        weight = full[half, pair, :, :, DOWN_AT + low : DOWN_AT + high]
        return dot_nt(hidden[:, low:high], weight.reshape(512, high - low))

    def down_early(i, _):
        half = lax.rem(1 - tp + i // 2, 2)
        partial[i] = down_part(half, lax.rem(i, 2), late, FF)
        g.steps_in(i, "downa")
        return 0

    g.gathered(2, (2, 3))
    g.steps("got2a")
    lax.fori_loop(0, 4, down_early, 0)
    g.gathered(2, (0, 1))

    def down_theirs(j, _):
        down_out[j] = (partial[j] + down_part(1 - tp, j, 0, late)).astype(BF16)
        to_partner(down_out.at[j], down_in.at[j], 9 + j).start()
        return 0

    lax.fori_loop(0, 2, down_theirs, 0)

    def down_mine(j, _):
        mine = (partial[j + 2] + down_part(tp, j, 0, late)).astype(BF16).astype(F32)
        to_partner(down_out.at[j], down_in.at[j], 9 + j).wait_recv()
        cols = pl.ds(pl.multiple_of(j * 512, 512), 512)
        summed = mine + down_in[j].astype(F32)
        out[:, cols] = (tok[tp, :, cols].astype(F32) + summed).astype(BF16)
        return 0

    lax.fori_loop(0, 2, down_mine, 0)
    for j in range(8):
        to_partner(mix_out.at[j], mix_in.at[j], 1 + j).wait_send()
    for j in range(2):
        to_partner(down_out.at[j], down_in.at[j], 9 + j).wait_send()
    g.leave()


def local(
    tokens,
    first_norm_gain,
    query_projection_weight,
    key_projection_weight,
    value_projection_weight,
    output_gate_weight,
    decay_projection_weight,
    fading_shift_vector,
    added_fading_exponent,
    per_head_gain,
    mixer_result_matrix,
    second_norm_gain,
    up_linear_weight,
    up_gating_weight,
    depthwise_taps,
    depthwise_bias,
    down_projection_weight,
):
    any_spec = pl.BlockSpec(memory_space=pl.ANY)
    vmem_spec = pl.BlockSpec(memory_space=pltpu.VMEM)
    dma = pltpu.SemaphoreType.DMA
    return pl.pallas_call(
        layer_kernel,
        out_shape=pltpu.VMEM((ROWS, HALF), BF16),
        in_specs=[any_spec] * 11 + [vmem_spec] * 6,
        out_specs=vmem_spec,
        scratch_shapes=[
            pltpu.VMEM((2, 4, 4, 64, COLS), BF16),
            pltpu.VMEM((8, 2048), F32),
            pltpu.VMEM((2, ROWS, HALF), BF16),
            pltpu.VMEM((ROWS, 2048), BF16),
            pltpu.VMEM((ROWS, 1536), BF16),
            pltpu.VMEM((ROWS, 256), F32),
            pltpu.VMEM((ROWS, 256), F32),
            pltpu.VMEM((ROWS, 512), BF16),
            pltpu.VMEM((8, ROWS, 256), BF16),
            pltpu.VMEM((8, ROWS, 256), BF16),
            pltpu.VMEM((ROWS, FF), BF16),
            pltpu.VMEM((2, ROWS, 512), BF16),
            pltpu.VMEM((2, ROWS, 512), BF16),
            pltpu.VMEM((4, ROWS, 512), F32),
            dma((NSEM,)),
            dma((NSEM,)),
            dma((21,)),
            dma((11,)),
            dma((11,)),
        ],
        compiler_params=pltpu.CompilerParams(
            collective_id=0, has_side_effects=True, vmem_limit_bytes=LIMIT
        ),
        name="layer",
    )(
        tokens,
        query_projection_weight,
        key_projection_weight,
        value_projection_weight,
        output_gate_weight,
        decay_projection_weight,
        mixer_result_matrix.T,
        up_linear_weight,
        up_gating_weight,
        down_projection_weight.T,
        added_fading_exponent,
        first_norm_gain,
        fading_shift_vector[None],
        per_head_gain,
        second_norm_gain,
        depthwise_taps.transpose(1, 0, 2),
        depthwise_bias,
    )


def solution(mesh):
    return jax.shard_map(
        local,
        mesh=mesh,
        in_specs=(
            P(("rep", "fs"), "tp"),
            P(),
            P("fs", "tp"),
            P("fs", "tp"),
            P("fs", "tp"),
            P("fs", "tp"),
            P("fs", "tp"),
            P("tp"),
            P(("rep", "fs"), "tp"),
            P(),
            P("tp", "fs"),
            P(),
            P("fs", "tp"),
            P("fs", "tp"),
            P(None, None, "tp"),
            P(None, "tp"),
            P("tp", "fs"),
        ),
        out_specs=P(("rep", "fs"), "tp"),
        check_vma=False,
    )
```

```python
import jax
import jax.numpy as jnp
from jax import lax
from jax.experimental import pallas as pl
from jax.experimental.pallas import tpu as pltpu
from jax.sharding import PartitionSpec as P

LANE = 128
MESH = pl.DeviceIdType.MESH
GROUPS = ((0, (6, 6, 3, 3)), (18, (8, 8, 4, 4)), (42, (3, 3, 3, 3)))
COLS = 54 * LANE
CLASSES = (("x", 1, True), ("y", -1, True), ("x", 1, False), ("y", -1, False))
NSEM = 168


class Gather:
    def __init__(self, full, send_sem, recv_sem):
        self.full, self.send_sem, self.recv_sem = full, send_sem, recv_sem
        rep, fs, self.tp = (lax.axis_index(a) for a in ("rep", "fs", "tp"))
        self.x, self.y, self.l = lax.rem(fs, 4), lax.rem(fs // 4, 4), fs // 16
        self.z = rep * 2 + self.l
        self.ids, self.sent = {}, {}

    def device(self, dim, step):
        x, y, z = self.x, self.y, self.z
        if dim == "x":
            x = lax.rem(x + step + 4, 4)
        elif dim == "y":
            y = lax.rem(y + step + 4, 4)
        else:
            z = lax.rem(z + step + 4, 4)
        return (z // 2, lax.rem(z, 2) * 16 + y * 4 + x, self.tp)

    def neighbours(self):
        return [self.device(d, s) for d in "xyz" for s in (1, -1)] + [
            (self.z // 2, self.l * 16 + self.y * 4 + self.x, 1 - self.tp)
        ]

    def cols(self, g, c):
        at, widths = GROUPS[g]
        return pl.ds((at + sum(widths[:c])) * LANE, widths[c] * LANE)

    def piece(self, g, c, stage, off, half=None, z=None):
        first, _, last = CLASSES[c]
        if z is None:
            zs = pl.ds(self.l, 1) if last else pl.ds(0, 2)
        else:
            zs = pl.ds(z, 1)
        rows = pl.ds(0, 64) if half is None else pl.ds(32 * half, 32)
        dim = first if stage == 1 else ("y" if first == "x" else "x")
        mine = self.x if dim == "x" else self.y
        at = pl.ds(lax.rem(mine + off + 4, 4), 1)
        if stage == 1:
            other = pl.ds(self.y if dim == "x" else self.x, 1)
        else:
            other = pl.ds(0, 4)
        yx = (other, at) if dim == "x" else (at, other)
        return self.full.at[zs, yx[0], yx[1], rows, self.cols(g, c)]

    def copy(self, key, ref, dim, step):
        i = self.ids.setdefault(key, len(self.ids))
        return pltpu.make_async_remote_copy(
            src_ref=ref,
            dst_ref=ref,
            send_sem=self.send_sem.at[i],
            recv_sem=self.recv_sem.at[i],
            device_id=self.device(dim, step),
            device_id_type=MESH,
        )

    def send(self, key, ref_args, dim, step):
        copy = self.copy(key, self.piece(*ref_args), dim, step)
        copy.start()
        self.sent[key] = (ref_args, dim, step)

    def recv(self, key, ref):
        self.copy(key, ref, "x", 1).wait_recv()

    def dim(self, c, stage):
        first = CLASSES[c][0]
        return first if stage == 1 else ("y" if first == "x" else "x")

    def hop_one(self, g, c, stage):
        d = self.dim(c, stage)
        for late in range(stage):
            for name, first, to in (("f1", 0, 1), ("b1", 1, -1)):
                half = None if stage == 1 else (first + late) % 2
                self.send((g, c, stage, name, late), (g, c, stage, 0, half), d, to)

    def hop_two(self, g, c, stage):
        d = self.dim(c, stage)
        for name, onward, half, off in (("f1", "f2", 0, -1), ("b1", "b2", 1, 1)):
            whole = None if stage == 1 else half
            self.recv((g, c, stage, name, 0), self.piece(g, c, stage, off, whole))
            self.send((g, c, stage, onward), (g, c, stage, off, half), d, -off)
        if CLASSES[c][2]:
            self.hop_rest(g, c, stage)

    def hop_rest(self, g, c, stage):
        if stage == 2:
            self.recv((g, c, stage, "f1", 1), self.piece(g, c, stage, -1, 1))
            self.recv((g, c, stage, "b1", 1), self.piece(g, c, stage, 1, 0))

    def hop_end(self, g, c, stage):
        if not CLASSES[c][2]:
            self.hop_rest(g, c, stage)
        self.recv((g, c, stage, "f2"), self.piece(g, c, stage, 2, 0))
        self.recv((g, c, stage, "b2"), self.piece(g, c, stage, 2, 1))

    def zkey(self, g, c, stage, off):
        return (g, c, stage, "z", off)

    def zsend(self, g, c, stage, off):
        self.send(
            self.zkey(g, c, stage, off),
            (g, c, stage, off, None, self.l),
            "z",
            CLASSES[c][1],
        )

    def zrecv(self, g, c, stage, off):
        self.recv(
            self.zkey(g, c, stage, off), self.piece(g, c, stage, off, z=1 - self.l)
        )

    def unit(self, g, c, k):
        last = CLASSES[c][2]
        if k == 0:
            if last:
                self.hop_one(g, c, 1)
            self.zsend(g, c, 1, 0)
        elif k == 1:
            self.zrecv(g, c, 1, 0)
            self.hop_one(g, c, 1)
        elif k in (2, 3, 6, 7):
            stage = 1 if k < 4 else 2
            self.hop_two(g, c, stage)
            if last:
                self.zsend(g, c, stage, -1)
                self.zsend(g, c, stage, 1)
        elif k in (4, 5):
            self.hop_end(g, c, 1)
            self.hop_one(g, c, 2)
            if last:
                self.zsend(g, c, 1, 2)
        elif k == 8:
            self.hop_end(g, c, 2)
            self.zsend(g, c, 2, 2)

    def gathered(self, g, classes=(2, 3, 0, 1)):
        for c in classes:
            if not CLASSES[c][2]:
                self.hop_end(g, c, 2)
                continue
            for off in (0, -1, 1, 2):
                self.zrecv(g, c, 1, off)
            for off in (-1, 1, 2):
                self.zrecv(g, c, 2, off)

    def enter(self):
        barrier = pltpu.get_barrier_semaphore()
        for d in self.neighbours():
            pl.semaphore_signal(barrier, inc=1, device_id=d, device_id_type=MESH)
        pl.semaphore_wait(barrier, 7)

    def partner(self):
        return (self.z // 2, self.l * 16 + self.y * 4 + self.x, 1 - self.tp)

    def steps(self, phase, i=0):
        for todo in PLAN.get(phase, {}).get(i, ()):
            self.unit(*todo)

    def steps_in(self, i, phase, every=1, start=0, stop=99):
        for at in sorted(set(PLAN.get(phase, {})) & set(range(start, stop))):

            @pl.when(i == at * every + every - 1)
            def _():
                self.steps(phase, at)

    def leave(self):
        for key, (ref_args, dim, step) in self.sent.items():
            self.copy(key, self.piece(*ref_args), dim, step).wait_send()


LIMIT = 65011712
ROWS = 768
SEQ = 256
HALF = 1024
NORM_EPS = 1e-06
VALUE_DIM = 128
SHARPNESS = 16.0
MIX_AT, UP_AT, DOWN_AT, FF = 1792, 2304, 5376, 1536
ROW_STEP = 128
PER_UNIT = ROWS // ROW_STEP // 6
F32, BF16 = jnp.float32, jnp.bfloat16

PLAN = {
    'open': {
        0: [(0, 2, 0), (0, 0, 0), (2, 2, 0), (0, 3, 0), (0, 1, 0)],
    },
    'norm': {
        0: [(1, 1, 0), (2, 3, 0), (1, 2, 0), (1, 3, 0), (2, 1, 0), (1, 0, 0), (2, 0, 0)],
        1: [(0, 0, 2), (0, 3, 1)],
        2: [(0, 1, 2), (0, 2, 1), (1, 2, 1), (1, 1, 2)],
        3: [(0, 0, 4), (0, 1, 4), (1, 2, 3), (0, 2, 3), (1, 0, 2), (1, 3, 1), (0, 3, 3), (0, 0, 6), (0, 1, 6), (0, 3, 5), (0, 2, 5), (1, 3, 3), (1, 0, 4), (1, 1, 4), (0, 1, 8), (0, 2, 7), (0, 0, 8), (0, 3, 7), (2, 3, 1), (2, 2, 1), (2, 0, 2), (1, 0, 6)],
        4: [(2, 1, 2), (1, 1, 6)],
    },
    'got0': {
        0: [(1, 2, 5), (1, 3, 5)],
    },
    'heads': {
        1: [(2, 3, 3)],
        2: [(1, 1, 8)],
        3: [(1, 2, 7), (1, 3, 7), (2, 2, 3)],
        5: [(1, 0, 8)],
    },
    'mix': {
        0: [(2, 1, 4)],
        1: [(2, 0, 4)],
        6: [(2, 3, 5)],
    },
    'second': {
        4: [(2, 2, 5)],
    },
    'up': {
        1: [(2, 0, 6)],
        2: [(2, 3, 7), (2, 2, 7)],
        4: [(2, 0, 8), (2, 1, 8)],
    },
    'got1b': {
        0: [(2, 1, 6)],
    },
}


def dot(a, b):
    return jnp.dot(a, b, preferred_element_type=F32)


def dot_nt(a, b):
    return lax.dot_general(a, b, (((1,), (1,)), ((), ())), preferred_element_type=F32)


def normalize(parts, gain_ref):
    total = sum(jnp.sum(p * p, axis=-1, keepdims=True) for p in parts)
    scale = lax.rsqrt(total * (1.0 / 2048) + NORM_EPS)
    width = 2048 // len(parts)
    return [
        (p * scale * gain_ref[:, i * width : (i + 1) * width]).astype(BF16)
        for i, p in enumerate(parts)
    ]


def head_pair(s, pair, qkvg, decay, mixed, head_gain):
    rows = pl.ds(pl.multiple_of(s * SEQ, SEQ), SEQ)
    at = pl.multiple_of(pair * LANE, LANE)
    lane = lax.broadcasted_iota(jnp.int32, (1, LANE), 1)
    low = lane < 64
    t = lax.broadcasted_iota(jnp.int32, (SEQ, SEQ), 0)
    u = lax.broadcasted_iota(jnp.int32, (SEQ, SEQ), 1)
    before = u <= t
    after = u >= t

    log_a = decay[rows, pl.ds(at, LANE)]
    ones = before.astype(F32).astype(BF16)
    high = log_a.astype(BF16)
    rest = log_a - high.astype(F32)
    middle = rest.astype(BF16)
    small = (rest - middle.astype(F32)).astype(BF16)
    done = dot(ones, high) + (dot(ones, middle) + dot(ones, small))
    open_ = done - log_a
    mid = [done[64 * b + 31 : 64 * b + 32] for b in range(4)]
    mid_open = [open_[64 * b + 32 : 64 * b + 33] for b in range(4)]

    q = qkvg[rows, pl.ds(at, LANE)].astype(F32) * 0.125
    k = qkvg[rows, pl.ds(pl.multiple_of(at + 256, LANE), LANE)].astype(F32)
    blocks = [slice(64 * b, 64 * b + 64) for b in range(4)]
    key_fwd = [k[r] * jnp.exp(mid[b] - done[r]) for b, r in enumerate(blocks)]
    key_bwd = [k[r] * jnp.exp(open_[r] - mid_open[b]) for b, r in enumerate(blocks)]

    def swap(v):
        return pltpu.roll(v, 64, 1)

    def both(v, parity):
        other = swap(v)
        return jnp.where(low, v, other) if parity == 0 else jnp.where(low, other, v)

    nothing = jnp.zeros((64, LANE), BF16)

    def side(queries, points, mids, keys, backward, parity):
        sign = -1.0 if backward else 1.0
        point_mids = [
            jnp.where(low, both(mids[2 * p], parity), both(mids[2 * p + 1], parity))
            for p in range(2)
        ]
        left, right = [], []
        for b, r in enumerate(blocks):
            row = []
            for p in range(2):
                expo = (points[r] - point_mids[p]) * sign
                if backward:
                    used = (b <= 2 * p, b <= 2 * p + 1)
                else:
                    used = (b >= 2 * p, b >= 2 * p + 1)
                if not any(used):
                    row.append(nothing)
                    continue
                if not all(used):
                    expo = jnp.where(low if used[0] else ~low, expo, -1e30)
                row.append((queries[r] * jnp.exp(expo)).astype(BF16))
            left.append(jnp.concatenate(row, axis=1))
            mine = keys[b] if parity == b % 2 else swap(keys[b])
            mine = jnp.where(low if b % 2 == 0 else ~low, mine, 0.0).astype(BF16)
            right.append(
                jnp.concatenate([mine if p == b // 2 else nothing for p in range(2)], axis=1)
            )
        return dot_nt(jnp.concatenate(left, axis=0), jnp.concatenate(right, axis=0))

    for parity in range(2):
        queries = both(q, parity)
        fwd = side(queries, both(done, parity), mid, key_fwd, False, parity)
        bwd = side(queries, both(open_, parity), mid_open, key_bwd, True, parity)
        scores = jnp.where(before, fwd, 0.0) + jnp.where(after, bwd, 0.0)
        place = pl.multiple_of(pair * 256 + parity * LANE, LANE)
        values = qkvg[rows, pl.ds(pl.multiple_of(place + 512, LANE), LANE)]
        out = dot(scores.astype(BF16), values)
        scale = lax.rsqrt(jnp.mean(out * out, axis=-1, keepdims=True) + NORM_EPS)
        out = out * scale * head_gain[...]
        gate = qkvg[rows, pl.ds(pl.multiple_of(place + 1024, LANE), LANE)].astype(F32)
        out = out * (gate * jax.nn.sigmoid(gate))
        mixed[rows, pl.ds(place, LANE)] = out.astype(BF16)


def smooth(source, taps, bias):
    row = lax.broadcasted_iota(jnp.int32, source.shape, 0)
    back = jnp.where(row == 0, 0.0, pltpu.roll(source, 1, 0))
    ahead = jnp.where(row == SEQ - 1, 0.0, pltpu.roll(source, SEQ - 1, 0))
    return bias + back * taps[0:1] + source * taps[1:2] + ahead * taps[2:3]


def layer_kernel(
    tokens,
    wq,
    wk,
    wv,
    wg,
    wd,
    mix_t,
    up_lin,
    up_gate,
    down_t,
    added,
    gain_one,
    shift,
    head_gain,
    gain_two,
    taps,
    bias,
    out,
    full,
    gains,
    tok,
    normed,
    qkvg,
    decay,
    fading,
    mixed,
    mix_out,
    mix_in,
    hidden,
    down_out,
    down_in,
    partial,
    send_sem,
    recv_sem,
    load_sem,
    pair_send,
    pair_recv,
):
    g = Gather(full, send_sem, recv_sem)
    tp = g.tp
    own = full.at[g.l, g.y, g.x]
    loads = [pltpu.make_async_copy(tokens, tok.at[tp], load_sem.at[0])]
    parts = [(w, 0, w.shape[1]) for w in (wq, wk, wv, wg, wd, mix_t)]
    parts += [(w, at, 256) for at in range(0, FF, 256) for w in (up_lin, up_gate)]
    parts += [(down_t, 0, FF)]
    at = 0
    for n, (w, first, width) in enumerate(parts):
        loads.append(
            pltpu.make_async_copy(
                w.at[:, pl.ds(first, width)], own.at[:, pl.ds(at, width)], load_sem.at[n + 1]
            )
        )
        at += width
    fading_load = pltpu.make_async_copy(added, fading, load_sem.at[20])
    for load in loads:
        load.start()
    fading_load.start()
    gains[0:1] = gain_one[...].astype(F32)[None]
    gains[1:2] = gain_two[...].astype(F32)[None]
    gains[2:3, :VALUE_DIM] = head_gain[...].astype(F32)[None]
    gain_one, gain_two = gains.at[0:1], gains.at[1:2]
    head_gain = gains.at[2:3, :VALUE_DIM]
    g.enter()

    def to_partner(src, dst, n):
        return pltpu.make_async_remote_copy(
            src_ref=src,
            dst_ref=dst,
            send_sem=pair_send.at[n],
            recv_sem=pair_recv.at[n],
            device_id=g.partner(),
            device_id_type=MESH,
        )

    for load in loads[1:]:
        load.wait()
    opening = PLAN["open"][0]
    sends = next((n for n, todo in enumerate(opening) if todo[2]), len(opening))
    for todo in opening[:sends]:
        g.unit(*todo)
    loads[0].wait()
    swap_tokens = to_partner(tok.at[tp], tok.at[tp], 0)
    swap_tokens.start()
    for todo in opening[sends:]:
        g.unit(*todo)
    fading_load.wait()
    to_partner(tok.at[tp], tok.at[1 - tp], 0).wait_recv()

    def first_norm(i, _):
        rows = pl.ds(pl.multiple_of(i * ROW_STEP, ROW_STEP), ROW_STEP)
        parts = normalize([tok[h, rows, :].astype(F32) for h in range(2)], gain_one)
        for h in range(2):
            normed[rows, h * HALF : (h + 1) * HALF] = parts[h]
        g.steps_in(i, "norm", PER_UNIT)
        return 0

    lax.fori_loop(0, ROWS // ROW_STEP, first_norm, 0)
    g.gathered(0)
    g.steps("got0")

    score = dot(normed[...], full[:, :, :, :, 1536:1792].reshape(2048, 256)) + shift[...]
    faded = jnp.minimum(score, 0.0) - jnp.log1p(jnp.exp(-jnp.abs(score)))
    decay[...] = faded * (1.0 / SHARPNESS) + fading[...]

    g.steps("project")

    def project(j, _):
        cols = pl.ds(pl.multiple_of(j * 256, 256), 256)
        weight = full[:, :, :, :, cols].reshape(2048, 256)
        qkvg[:, cols] = dot(normed[...], weight).astype(BF16)
        g.steps_in(j + 1, "project", 1, 1)
        return 0

    lax.fori_loop(0, 6, project, 0)

    def heads(i, _):
        head_pair(i // 2, lax.rem(i, 2), qkvg, decay, mixed, head_gain)
        g.steps_in(i, "heads")
        return 0

    lax.fori_loop(0, 6, heads, 0)

    def mix(j, _):
        weight = full[j // 4, lax.rem(j, 4), :, :, MIX_AT:UP_AT].reshape(256, 512)
        mix_out[j] = dot_nt(mixed[...], weight).astype(BF16)
        to_partner(mix_out.at[j], mix_in.at[j], 1 + j).start()
        g.steps_in(j, "mix")
        return 0

    lax.fori_loop(0, 8, mix, 0)
    for j in range(8):
        to_partner(mix_out.at[j], mix_in.at[j], 1 + j).wait_recv()
    g.steps("mixed")

    def second_norm(i, _):
        rows = pl.ds(pl.multiple_of(i * ROW_STEP, ROW_STEP), ROW_STEP)
        parts = []
        for j in range(8):
            cols = slice((j % 4) * 256, (j % 4 + 1) * 256)
            term = mix_out[j, rows, :].astype(F32) + mix_in[j, rows, :].astype(F32)
            kept = (tok[j // 4, rows, cols].astype(F32) + term).astype(BF16)
            tok[j // 4, rows, cols] = kept
            parts.append(kept.astype(F32))
        for j, part in enumerate(normalize(parts, gain_two)):
            normed[rows, j * 256 : (j + 1) * 256] = part
        g.steps_in(i, "second", PER_UNIT)
        return 0

    swap_tokens.wait_send()
    lax.fori_loop(0, ROWS // ROW_STEP, second_norm, 0)
    def up(j, _):
        cols = pl.ds(pl.multiple_of(j * 256, 256), 256)
        at = pl.multiple_of(UP_AT + j * 512, 256)
        weight = full[:, :, :, :, pl.ds(at, 512)].reshape(2048, 512)
        both = dot(normed[...], weight).astype(BF16)
        parts = [both[:, :256], both[:, 256:]]
        tap = [taps[:, half, cols].astype(F32) for half in range(2)]
        base = bias[:, cols].astype(F32)
        for s in range(ROWS // SEQ):
            rows = slice(s * SEQ, (s + 1) * SEQ)
            lin, gate = (
                smooth(parts[h][rows].astype(F32), tap[h], base[h : h + 1]) for h in range(2)
            )
            hidden[rows, cols] = (lin * (gate * jax.nn.sigmoid(gate))).astype(BF16)
        return 0

    done = 0
    for phase, classes, chunks in (
        ("got1a", (2, 3), (4, 6)),
        ("got1b", (0,), (0, 2)),
        ("got1c", (1,), (2, 4)),
    ):
        g.gathered(1, classes)
        g.steps(phase)

        def piece(j, _, shift=done - chunks[0], at=done):
            up(j, 0)
            g.steps_in(j + shift, "up", 1, at, at + 2)
            return 0

        lax.fori_loop(*chunks, piece, 0)
        done += 2

    late = sum(GROUPS[2][1][:2]) * LANE

    def down_part(half, j, low, high):
        pair = pl.ds(pl.multiple_of(2 * j, 2), 2)
        weight = full[half, pair, :, :, DOWN_AT + low : DOWN_AT + high]
        return dot_nt(hidden[:, low:high], weight.reshape(512, high - low))

    def down_early(i, _):
        half = lax.rem(1 - tp + i // 2, 2)
        partial[i] = down_part(half, lax.rem(i, 2), late, FF)
        g.steps_in(i, "downa")
        return 0

    g.gathered(2, (2, 3))
    g.steps("got2a")
    lax.fori_loop(0, 4, down_early, 0)
    g.gathered(2, (0, 1))

    def down_theirs(j, _):
        down_out[j] = (partial[j] + down_part(1 - tp, j, 0, late)).astype(BF16)
        to_partner(down_out.at[j], down_in.at[j], 9 + j).start()
        return 0

    lax.fori_loop(0, 2, down_theirs, 0)

    def down_mine(j, _):
        mine = (partial[j + 2] + down_part(tp, j, 0, late)).astype(BF16).astype(F32)
        to_partner(down_out.at[j], down_in.at[j], 9 + j).wait_recv()
        cols = pl.ds(pl.multiple_of(j * 512, 512), 512)
        summed = mine + down_in[j].astype(F32)
        out[:, cols] = (tok[tp, :, cols].astype(F32) + summed).astype(BF16)
        return 0

    lax.fori_loop(0, 2, down_mine, 0)
    for j in range(8):
        to_partner(mix_out.at[j], mix_in.at[j], 1 + j).wait_send()
    for j in range(2):
        to_partner(down_out.at[j], down_in.at[j], 9 + j).wait_send()
    g.leave()


def local(
    tokens,
    first_norm_gain,
    query_projection_weight,
    key_projection_weight,
    value_projection_weight,
    output_gate_weight,
    decay_projection_weight,
    fading_shift_vector,
    added_fading_exponent,
    per_head_gain,
    mixer_result_matrix,
    second_norm_gain,
    up_linear_weight,
    up_gating_weight,
    depthwise_taps,
    depthwise_bias,
    down_projection_weight,
):
    any_spec = pl.BlockSpec(memory_space=pl.ANY)
    vmem_spec = pl.BlockSpec(memory_space=pltpu.VMEM)
    dma = pltpu.SemaphoreType.DMA
    return pl.pallas_call(
        layer_kernel,
        out_shape=pltpu.VMEM((ROWS, HALF), BF16),
        in_specs=[any_spec] * 11 + [vmem_spec] * 6,
        out_specs=vmem_spec,
        scratch_shapes=[
            pltpu.VMEM((2, 4, 4, 64, COLS), BF16),
            pltpu.VMEM((8, 2048), F32),
            pltpu.VMEM((2, ROWS, HALF), BF16),
            pltpu.VMEM((ROWS, 2048), BF16),
            pltpu.VMEM((ROWS, 1536), BF16),
            pltpu.VMEM((ROWS, 256), F32),
            pltpu.VMEM((ROWS, 256), F32),
            pltpu.VMEM((ROWS, 512), BF16),
            pltpu.VMEM((8, ROWS, 256), BF16),
            pltpu.VMEM((8, ROWS, 256), BF16),
            pltpu.VMEM((ROWS, FF), BF16),
            pltpu.VMEM((2, ROWS, 512), BF16),
            pltpu.VMEM((2, ROWS, 512), BF16),
            pltpu.VMEM((4, ROWS, 512), F32),
            dma((NSEM,)),
            dma((NSEM,)),
            dma((21,)),
            dma((11,)),
            dma((11,)),
        ],
        compiler_params=pltpu.CompilerParams(
            collective_id=0, has_side_effects=True, vmem_limit_bytes=LIMIT
        ),
        name="layer",
    )(
        tokens,
        query_projection_weight,
        key_projection_weight,
        value_projection_weight,
        output_gate_weight,
        decay_projection_weight,
        mixer_result_matrix.T,
        up_linear_weight,
        up_gating_weight,
        down_projection_weight.T,
        added_fading_exponent,
        first_norm_gain,
        fading_shift_vector[None],
        per_head_gain,
        second_norm_gain,
        depthwise_taps.transpose(1, 0, 2),
        depthwise_bias,
    )


def solution(mesh):
    return jax.shard_map(
        local,
        mesh=mesh,
        in_specs=(
            P(("rep", "fs"), "tp"),
            P(),
            P("fs", "tp"),
            P("fs", "tp"),
            P("fs", "tp"),
            P("fs", "tp"),
            P("fs", "tp"),
            P("tp"),
            P(("rep", "fs"), "tp"),
            P(),
            P("tp", "fs"),
            P(),
            P("fs", "tp"),
            P("fs", "tp"),
            P(None, None, "tp"),
            P(None, "tp"),
            P("tp", "fs"),
        ),
        out_specs=P(("rep", "fs"), "tp"),
        check_vma=False,
    )
```
